256 devices in a mesh: grp: 2 (over z), ep: 16 (over y, core), tp: 8 (over x).
Axes of the slice: x: 8, y: 8, z: 2, core: 2. Of those that a mesh axis runs over, the one named last changes fastest.
The devices are a block of a 8x8x16 slice.
Arguments:
- pool_input: bfloat16 [32768, 1024], P(('grp', 'ep'), 'tp'), parts along dimension 0, may hold values from -6 to 6
- pool_map: bfloat16 [8, 128, 128], replicated, may hold values from -0.5 to 0.5
- pool_scale: float32 [1024], replicated, may hold values from 0.1 to 1.9
- out_weight: bfloat16 [1024, 2048], P(None, 'tp'), may hold values from -0.1875 to 0.1875
- expert_input: bfloat16 [32768, 2048], P(('grp', 'ep', 'tp')), parts along dimension 0, may hold values from -6 to 6
- norm_gain: float32 [2048], replicated, may hold values from 0.1 to 1.9
- routes: int32 [32768, 2], P(('grp', 'ep', 'tp')), parts along dimension 0, may hold values from 0 to 127, all different within a row; in each aligned block of 128 rows (0 to 127, 128 to 255, ...) at most 4 rows name the same one
- route_weight: float32 [32768, 2], P(('grp', 'ep', 'tp')), parts along dimension 0, may hold values from 0.2 to 1.5
- gate_weight: bfloat16 [128, 2048, 512], P(('ep', 'tp')), may hold values from -0.125 to 0.125
- up_weight: bfloat16 [128, 2048, 512], P(('ep', 'tp')), may hold values from -0.125 to 0.125
- down_weight: bfloat16 [128, 512, 2048], P(('ep', 'tp')), may hold values from -0.25 to 0.25
Outputs:
- pool_output: bfloat16 [32768, 2048], P(('grp', 'ep'), 'tp'), parts along dimension 0
- expert_output: bfloat16 [32768, 2048], P(('grp', 'ep', 'tp')), parts along dimension 0
The draws below stay inside these ranges and needn't reach their ends.
There are 2 independent parts, one for each index of `grp`. The reference program is written for one: setup_inputs(seed, part) draws one part's arguments, and reference() takes and returns one part's arrays. A program takes and returns all parts, laid end to end along the dimension named above; an argument that names none is the same for every part. Nothing has to cross between parts.
Inputs may be any that keep to these rules, and one draw needn't show every extreme that they name: `routes`: each row names 2 different experts. In the rows of one device no expert is named more than 4 times, and in every draw some device names some expert exactly 4 times.
All inputs are finite; a program needn't handle non-finite values.
Results may differ from the reference program's by a relative error of at most 0.007.
Values may be sent and summed in bfloat16 or wider, within the bound.
A program may use at most 64 MiB of HBM per device.

```python
import math
import jax
import jax.numpy as jnp
import numpy as np
from jax import lax

D = 2048
D_EXPERT = 512
GROUP_DIM = 128
GROUPS = 8
TOP_K = 2
ROWS_B = 128
D_POOL = 1024
EXPERTS = 128
CAP = 4
TOKENS_A = 16384
TOKENS_B = 16384
N_EP = 16
N_TP = 8


def shard_levels(key, shape, split, low, top_value):
    loudness = 1.0
    for position, blocks in split:
        draws = jax.random.uniform(jax.random.fold_in(jax.random.fold_in(key, 6), position), (blocks,), jnp.float32, low / len(split), top_value / len(split))
        loudness = loudness * jnp.repeat(jnp.exp(draws), shape[position] // blocks).reshape((-1,) + (1,) * (len(shape) - 1 - position))
    return loudness


def routed_block(key, own, number, rows, amount, top, bound, skew):
    sequence = jax.random.permutation(key, amount)
    heavy_load, common = shares(amount, rows * top, bound, skew, True), shares(amount, rows * top, bound, skew, False)
    places = jnp.arange(amount)

    def named(tallies, turn):
        used = int((tallies > 0).sum())
        fixed = max(1, used // 4)
        moved = fixed + (places - fixed + turn * (used - fixed)) % max(1, amount - fixed)
        return jnp.zeros((amount,), jnp.int32).at[sequence[jnp.where(places < fixed, places, moved)]].set(jnp.asarray(tallies, jnp.int32))

    tallies = jnp.where(number % 4 == 0, named(heavy_load, number // 4), named(common, number - number // 4 - 1))
    mixed = jax.random.permutation(jax.random.fold_in(own, 3), amount)
    giver, receiver = mixed[0:amount // 2 * 2:2], mixed[1:amount // 2 * 2:2]
    margin = jnp.minimum(tallies[giver] - 1, bound - tallies[receiver]) // 2
    margin = jnp.where((giver == sequence[0]) | (receiver == sequence[0]) | (tallies[receiver] == 0), 0, jnp.maximum(margin, 0))
    moved = jax.random.randint(jax.random.fold_in(own, 4), (amount // 2,), 0, 1 << 20) % (margin + 1)
    tallies = tallies.at[giver].add(-moved).at[receiver].add(moved)
    labels = jnp.searchsorted(jnp.cumsum(tallies), jnp.arange(rows * top), side="right").astype(jnp.int32)
    grid = labels.reshape(top, rows).T
    grid = grid[jax.random.permutation(jax.random.fold_in(own, 1), rows)]
    turn = jax.random.randint(jax.random.fold_in(own, 2), (rows, 1), 0, top)
    return jnp.take_along_axis(grid, (jnp.arange(top)[None, :] + turn) % top, axis=1)


def shares(amount, total, limit, skew, full):
    weights = [(1 << 20) // math.isqrt(standing ** skew) + 1 for standing in range(1, amount + 1)]
    largest = limit if full else min(limit, max(-(-total // amount), total * weights[0] // sum(weights)))
    least = 1 if total - largest >= amount - 1 else 0
    given, spare = [largest] + [least] * (amount - 1), total - largest - least * (amount - 1)
    while spare > 0:
        candidates = [i for i in range(1, amount) if given[i] < largest] or [i for i in range(1, amount) if given[i] < limit]
        whole, remaining = sum([weights[i] for i in candidates]), spare
        for i in candidates:
            more = min(limit - given[i], max(1, remaining * weights[i] // whole), spare)
            given[i] = given[i] + more
            spare = spare - more
    return np.array(given)


def scatter_about(stream_key, shape, width, bound, pieces=(), held_as=jnp.bfloat16):
    values = jax.random.normal(stream_key, shape, jnp.float32) * width
    if len(pieces) > 0:
        values = shard_levels(stream_key, shape, pieces, -0.22, 0.18) * values
    return jnp.clip(values, min=-bound, max=bound).astype(held_as)


def setup_inputs(seed: int = 0, part: int = 0) -> dict:
    seeds = jax.random.split(jax.random.key(seed), 12)
    part_splits = jax.random.split(jax.random.fold_in(seeds[11], part), 12)
    pool_input = scatter_about(part_splits[0], (TOKENS_A, D_POOL), 1.0, 6.0, ((0, 16), (1, 8)))
    pool_map = scatter_about(seeds[1], (GROUPS, GROUP_DIM, GROUP_DIM), GROUP_DIM ** -0.5, 0.5)
    pool_scale = jnp.clip(1.0 + 0.18 * jax.random.normal(seeds[2], (D_POOL,), jnp.float32), 0.1, 1.9)
    out_weight = scatter_about(seeds[3], (D_POOL, D), D_POOL ** -0.5, 0.1875, ((1, 8),))
    expert_input = scatter_about(part_splits[4], (TOKENS_B, D), 1.0, 6.0, ((0, 128),))
    norm_gain = jnp.clip(1.0 + 0.18 * jax.random.normal(seeds[5], (D,), jnp.float32), 0.1, 1.9)
    routes_keys = jax.random.split(jax.random.fold_in(part_splits[6], 1), TOKENS_B // ROWS_B)
    routes_turns = jax.random.permutation(jax.random.fold_in(part_splits[6], 3), TOKENS_B // ROWS_B)
    routes = jax.vmap(lambda own, number: routed_block(jax.random.fold_in(part_splits[6], 2), own, number, ROWS_B, EXPERTS, TOP_K, CAP, 2))(routes_keys, routes_turns).reshape((TOKENS_B, TOP_K))
    route_weight = jnp.clip(0.2 + 1.3 * jax.random.uniform(part_splits[7], (TOKENS_B, TOP_K), jnp.float32) ** shard_levels(part_splits[7], (TOKENS_B, TOP_K), ((0, 128),), -0.2, 0.2), 0.2, 1.5)
    gate_weight = scatter_about(seeds[8], (EXPERTS, D, D_EXPERT), D ** -0.5, 0.125, ((0, 128),))
    up_weight = scatter_about(seeds[9], (EXPERTS, D, D_EXPERT), D ** -0.5, 0.125, ((0, 128),))
    down_weight = scatter_about(seeds[10], (EXPERTS, D_EXPERT, D), D_EXPERT ** -0.5, 0.25, ((0, 128),))
    return {"pool_input": pool_input, "pool_map": pool_map, "pool_scale": pool_scale, "out_weight": out_weight, "expert_input": expert_input, "norm_gain": norm_gain, "routes": routes, "route_weight": route_weight, "gate_weight": gate_weight, "up_weight": up_weight, "down_weight": down_weight}


epsilon = 1e-06

def pool_group(column_block, window):
    length = column_block.shape[0]
    running = jnp.cumsum(column_block, axis=0)
    earlier = jnp.pad(running, ((window, 0), (0, 0)))[:length]
    counted = jnp.minimum(jnp.arange(length) + 1, window).astype(jnp.float32)
    return (running - earlier) / counted[:, None] - column_block

def reference(pool_input, pool_map, pool_scale, out_weight, expert_input, norm_gain, routes, route_weight, gate_weight, up_weight, down_weight):
    widened = pool_input.astype(jnp.float32)
    mapped_parts = []
    for group_index in range(GROUPS):
        window = 2 ** (1 + group_index % 4)
        lower = group_index * GROUP_DIM
        columns = widened[:, lower:lower + GROUP_DIM]
        pooled = pool_group(columns, window).astype(jnp.bfloat16)
        mapped = jnp.dot(pooled, pool_map[group_index], preferred_element_type=jnp.float32)
        mapped = mapped * pool_scale[lower:lower + GROUP_DIM]
        mapped_parts.append(mapped.astype(jnp.bfloat16))
    mapped_all = jnp.concatenate(mapped_parts, axis=1)
    pool_output = jnp.dot(mapped_all, out_weight, preferred_element_type=jnp.float32).astype(jnp.bfloat16)
    widened_b = expert_input.astype(jnp.float32)
    normed = widened_b * lax.rsqrt(lax.optimization_barrier(jnp.mean(widened_b * widened_b, axis=1, keepdims=True)) + epsilon) * norm_gain
    normed = normed.astype(jnp.bfloat16)
    devices_all = N_EP * N_TP
    copies = ROWS_B * TOP_K
    flat_routes = routes.reshape(devices_all, copies).astype(jnp.int32)
    onehot = (flat_routes[:, :, None] == jnp.arange(EXPERTS, dtype=jnp.int32)[None, None, :]).astype(jnp.int32)
    before = jnp.cumsum(onehot, axis=1) - onehot
    slot_index = lax.optimization_barrier(jnp.sum(before * onehot, axis=2)).astype(jnp.int32)
    device_of = jnp.arange(devices_all, dtype=jnp.int32)[:, None]
    target = (flat_routes * (devices_all * CAP) + device_of * CAP + slot_index).astype(jnp.int32)
    token_of = (device_of * ROWS_B + jnp.arange(copies, dtype=jnp.int32)[None, :] // TOP_K).astype(jnp.int32)
    slot_count = EXPERTS * devices_all * CAP
    slot_table = jnp.full((slot_count,), TOKENS_B, jnp.int32).at[target.reshape(-1)].set(token_of.reshape(-1))
    slot_weight = jnp.zeros((slot_count,), jnp.float32).at[target.reshape(-1)].set(route_weight.astype(jnp.float32).reshape(-1))
    padded = jnp.concatenate([normed, jnp.zeros((1, D), jnp.bfloat16)], axis=0)

    def one_expert(accumulated, inputs):
        tokens_here, weights_here, gate_here, up_here, down_here = inputs
        rows_here = padded[tokens_here]
        gate_part = jnp.dot(rows_here, gate_here, preferred_element_type=jnp.float32)
        up_part = jnp.dot(rows_here, up_here, preferred_element_type=jnp.float32)
        hidden = (jax.nn.silu(gate_part) * up_part).astype(jnp.bfloat16)
        result = jnp.dot(hidden, down_here, preferred_element_type=jnp.float32).astype(jnp.bfloat16)
        accumulated = accumulated.at[tokens_here].add(weights_here[:, None] * result.astype(jnp.float32))
        return (accumulated, None)
    initial = jnp.zeros((TOKENS_B + 1, D), jnp.float32)
    accumulated, unused = lax.scan(one_expert, initial, (slot_table.reshape(EXPERTS, -1), slot_weight.reshape(EXPERTS, -1), gate_weight, up_weight, down_weight))
    expert_output = accumulated[:TOKENS_B].astype(jnp.bfloat16)
    return (pool_output, expert_output)
```

```python
import functools

import jax
import jax.numpy as jnp
from jax import lax
from jax.experimental import pallas as pl
from jax.experimental.pallas import tpu as pltpu
from jax.sharding import PartitionSpec as P

MESH = pl.DeviceIdType.MESH
epsilon = 1e-06
halo_depth = 16
block_rows = 16


def dot32(a, b):
    return jnp.dot(a, b, preferred_element_type=jnp.float32)


def iota(shape, dim):
    return lax.broadcasted_iota(jnp.int32, shape, dim)


def ones_where(mask):
    return jnp.where(mask, 1.0, 0.0).astype(jnp.bfloat16)


def kernel(
    n_ep,
    n_tp,
    cap,
    x_hbm,
    gain_ref,
    routes_ref,
    routes_t_ref,
    weight_ref,
    gate_hbm,
    up_hbm,
    down_hbm,
    pool_hbm,
    map_hbm,
    scale_ref,
    proj_hbm,
    pool_out,
    expert_out,
    x_v,
    gate_v,
    up_v,
    down_v,
    pool_v,
    map_v,
    proj_v,
    halo_v,
    stacked,
    xs,
    xd,
    yd,
    ys,
    yr,
    xr,
    rows_v,
    perm,
    perm_t,
    total,
    ext,
    sums,
    gathered,
    local_sem,
    halo_sem,
    xs_sem,
    xd_sem,
    yf_sem,
    yd_sem,
    ys_sem,
    yr_sem,
    xb_sem,
    xr_sem,
    ring_send,
    ring_recv,
):
    ep = lax.axis_index("ep")
    tp = lax.axis_index("tp")
    half = n_tp // 2
    rows, width = x_v.shape
    quarters = block_rows // cap
    lanes = width // quarters
    span = n_ep * block_rows
    part = n_ep * cap

    def offset(b, h):
        return (b + 1) % half if h == 0 else n_tp - (b + 1)

    def twin(b, h):
        return 2 * b + (1 - h) if b < half - 1 else 2 * b + h

    barrier = pltpu.get_barrier_semaphore()
    for r in range(1, n_tp):
        pl.semaphore_signal(
            barrier, inc=1, device_id={"tp": lax.rem(tp + r, n_tp)}, device_id_type=MESH
        )

    def greet(r, carry):
        pl.semaphore_signal(
            barrier, inc=1, device_id={"ep": lax.rem(ep + r, n_ep)}, device_id_type=MESH
        )
        return carry

    lax.fori_loop(1, n_ep, greet, 0)

    loads = [
        pltpu.make_async_copy(x_hbm, x_v, local_sem.at[0]),
        pltpu.make_async_copy(pool_hbm, pool_v, local_sem.at[1]),
        pltpu.make_async_copy(map_hbm.at[tp], map_v, local_sem.at[2]),
        pltpu.make_async_copy(gate_hbm.at[0], gate_v, local_sem.at[3]),
        pltpu.make_async_copy(up_hbm.at[0], up_v, local_sem.at[4]),
        pltpu.make_async_copy(down_hbm.at[0], down_v, local_sem.at[5]),
        pltpu.make_async_copy(proj_hbm, proj_v, local_sem.at[6]),
    ]
    for load in loads:
        load.start()

    later = ones_where(iota((rows, rows), 0) < iota((rows, rows), 1))
    earlier = ones_where(iota((rows, rows), 0) > iota((rows, rows), 1))
    row_id, col_id = iota((span, span), 0), iota((span, span), 1)

    def home(v):
        return ((v // cap) % n_ep) * block_rows + (v // part) * cap + v % cap

    perm[...] = ones_where(home(row_id) == col_id)
    perm_t[...] = ones_where(row_id == home(col_id))

    loads[0].wait()
    widened = x_v[...].astype(jnp.float32)
    normed = (
        widened
        * lax.rsqrt(jnp.mean(widened * widened, axis=1, keepdims=True) + epsilon)
        * gain_ref[...]
    ).astype(jnp.bfloat16)
    for q in range(quarters):
        stacked[q * rows : (q + 1) * rows, :] = normed[:, q * lanes : (q + 1) * lanes]

    slot_row = iota((span, rows), 0)

    def build(slot, off):
        expert = (slot_row // block_rows) * n_tp + lax.rem(tp + off, n_tp)
        named = (routes_t_ref[0:1, :] == expert) | (routes_t_ref[1:2, :] == expert)
        before = dot32(ones_where(named), later)
        chosen = named & (before == (slot_row % cap).astype(jnp.float32))
        quarter = (slot_row // cap) % quarters
        selector = jnp.concatenate(
            [ones_where(chosen & (quarter == q)) for q in range(quarters)], axis=1
        )
        block = dot32(selector, stacked[...]).astype(jnp.bfloat16)
        xs[slot] = block.reshape(n_ep, block_rows, lanes)

    def send_x(b, h):
        pltpu.make_async_remote_copy(
            src_ref=xs.at[2 * b + h],
            dst_ref=xd.at[twin(b, h)],
            send_sem=xs_sem,
            recv_sem=xd_sem.at[twin(b, h)],
            device_id={"tp": lax.rem(tp + offset(b, h), n_tp)},
            device_id_type=MESH,
        ).start()

    def forward_y(slot, b, source):
        def one(r, carry):
            peer = lax.rem(ep + r, n_ep)
            pltpu.make_async_remote_copy(
                src_ref=source.at[slot, peer],
                dst_ref=yd.at[slot, ep],
                send_sem=yf_sem,
                recv_sem=yd_sem.at[b],
                device_id={"ep": peer},
                device_id_type=MESH,
            ).start()
            return carry

        lax.fori_loop(1, n_ep, one, 0)
        yd[slot, ep] = source[slot, ep]

    def wait_bytes(ref, sem):
        pltpu.make_async_copy(ref, ref, sem).wait()

    own = 2 * (half - 1)
    order = [(b, h) for b in range(half) for h in range(2) if 2 * b + h != own]
    build(2 * order[0][0] + order[0][1], offset(*order[0]))
    pl.semaphore_wait(barrier, n_tp - 1 + n_ep - 1)
    halo = pltpu.make_async_remote_copy(
        src_ref=pool_v.at[pool_v.shape[0] - halo_depth :],
        dst_ref=halo_v,
        send_sem=halo_sem.at[0],
        recv_sem=halo_sem.at[1],
        device_id={"ep": lax.rem(ep + 1, n_ep)},
        device_id_type=MESH,
    )
    build(2 * order[1][0] + order[1][1], offset(*order[1]))
    send_x(*order[0])
    build(own, 0)
    send_x(*order[1])
    loads[1].wait()
    halo.start()
    for n, (b, h) in enumerate(order[2:]):
        build(2 * b + h, offset(b, h))
        if n == 0:
            forward_y(own, half - 1, xs)
        else:
            send_x(*order[n + 1])
    send_x(*order[-1])

    loads[2].wait()
    positions, channels = pool_v.shape
    ext[halo_depth:, :] = pool_v[...].astype(jnp.float32)
    halo.wait_recv()
    halo_rows = halo_v[...].astype(jnp.float32)
    ext[0:halo_depth, :] = jnp.where(ep == 0, jnp.zeros_like(halo_rows), halo_rows)
    level = lax.rem(tp, 4)
    summed = ext[halo_depth:, :] + ext[halo_depth - 1 : -1, :]
    sums[0, halo_depth:, :] = summed
    sums[0, 1:halo_depth, :] = ext[1:halo_depth, :] + ext[0 : halo_depth - 1, :]
    reach = 2
    first = 1
    for n in range(3):
        first = first + reach
        wider = sums[n, first:, :] + sums[n, first - reach : -reach, :]
        if n < 2:
            sums[n + 1, first:, :] = wider
        summed = jnp.where(level > n, wider[halo_depth - first :], summed)
        reach = 2 * reach
    window = jnp.left_shift(2, level)
    position = ep * positions + iota((positions, channels), 0)
    counted = jnp.minimum(position + 1, window).astype(jnp.float32)
    pooled = (summed / counted - ext[halo_depth:, :]).astype(jnp.bfloat16)
    mapped = dot32(pooled, map_v[...]) * scale_ref[tp]
    gathered[tp] = mapped.astype(jnp.bfloat16)

    def ring(step, way):
        block = lax.rem(tp + n_tp - way * (step - 1), n_tp)
        lane = (1 - way) // 2
        return pltpu.make_async_remote_copy(
            src_ref=gathered.at[block],
            dst_ref=gathered.at[block],
            send_sem=ring_send.at[lane, step - 1],
            recv_sem=ring_recv.at[lane, step - 1],
            device_id={"tp": lax.rem(tp + n_tp + way, n_tp)},
            device_id_type=MESH,
        )

    def relay(b):
        for h in range(2):
            wait_bytes(xd.at[2 * b + h], xd_sem.at[2 * b + h])
            forward_y(2 * b + h, b, xd)

    relay(0)
    for load in loads[3:6]:
        load.wait()
    ring(1, 1).start()
    ring(1, -1).start()

    def send_back(b, last):
        for h in range(2):
            slot = 2 * b + h
            if last and slot == own:
                continue
            target = slot if last else 2 * b + (1 - h)
            off = half * h if last else (b + 1 if h == 0 else n_tp - 1 - b)
            pltpu.make_async_remote_copy(
                src_ref=yr.at[slot],
                dst_ref=xr.at[target],
                send_sem=xb_sem,
                recv_sem=xr_sem.at[target],
                device_id={"tp": lax.rem(tp + off, n_tp)},
                device_id_type=MESH,
            ).start()

    def experts(b, carry):
        @pl.when(b < half - 2)
        def _():
            for h in range(2):
                slot = 2 * (b + 1) + h
                wait_bytes(xd.at[slot], xd_sem.at[slot])
                forward_y(slot, b + 1, xd)

        @pl.when(b == half - 2)
        def _():
            wait_bytes(xd.at[own + 1], xd_sem.at[own + 1])
            forward_y(own + 1, half - 1, xd)

        wait_bytes(yd.at[pl.ds(2 * b, 2), pl.ds(0, n_ep - 1)], yd_sem.at[b])
        for h in range(2):
            block = yd[2 * b + h].reshape(span, lanes)
            ordered = dot32(perm[...], block).astype(jnp.bfloat16)
            for q in range(quarters):
                rows_v[h * part : (h + 1) * part, q * lanes : (q + 1) * lanes] = ordered[
                    q * part : (q + 1) * part, :
                ]
        gate = dot32(rows_v[...], gate_v[...])
        up = dot32(rows_v[...], up_v[...])
        hidden = (gate / (1.0 + jnp.exp(-gate)) * up).astype(jnp.bfloat16)
        result = dot32(hidden, down_v[...]).astype(jnp.bfloat16)
        for h in range(2):
            tall = jnp.concatenate(
                [
                    result[h * part : (h + 1) * part, q * lanes : (q + 1) * lanes]
                    for q in range(quarters)
                ],
                axis=0,
            )
            block = dot32(perm_t[...], tall).astype(jnp.bfloat16)
            ys[2 * b + h] = block.reshape(n_ep, block_rows, lanes)
        for h in range(2):
            yr[2 * b + h, ep] = ys[2 * b + h, ep]

        def one(r, c):
            peer = lax.rem(ep + r, n_ep)
            pltpu.make_async_remote_copy(
                src_ref=ys.at[pl.ds(2 * b, 2), peer],
                dst_ref=yr.at[pl.ds(2 * b, 2), ep],
                send_sem=ys_sem,
                recv_sem=yr_sem.at[b],
                device_id={"ep": peer},
                device_id_type=MESH,
            ).start()
            return c

        lax.fori_loop(1, n_ep, one, 0)

        @pl.when(b >= 1)
        def _():
            wait_bytes(yr.at[pl.ds(2 * (b - 1), 2), pl.ds(0, n_ep - 1)], yr_sem.at[b - 1])
            send_back(b - 1, False)

        ring(b + 1, 1).wait_recv()

        @pl.when(b < half - 1)
        def _():
            ring(b + 2, 1).start()
            ring(b + 1, -1).wait_recv()

        @pl.when(b < half - 2)
        def _():
            ring(b + 2, -1).start()

        return carry

    lax.fori_loop(0, half, experts, 0)
    wait_bytes(
        yr.at[pl.ds(own, 2), pl.ds(0, n_ep - 1)], yr_sem.at[half - 1]
    )
    send_back(half - 1, True)

    loads[6].wait()
    tile = positions // 4

    def project(n, carry):
        at = pl.ds(pl.multiple_of(n * tile, tile), tile)
        left = jnp.concatenate([gathered[j, at, :] for j in range(n_tp)], axis=1)
        pool_out[at, :] = dot32(left, proj_v[...]).astype(jnp.bfloat16)
        return carry

    lax.fori_loop(0, 4, project, 0)

    total[...] = jnp.zeros_like(total)
    lane_id = iota((rows, span), 1)

    def combine(off, source, slot):
        expert = (lane_id // block_rows) * n_tp + lax.rem(tp + off, n_tp)
        named_0 = routes_ref[:, 0:1] == expert
        named_1 = routes_ref[:, 1:2] == expert
        before = dot32(earlier, ones_where(named_0 | named_1))
        hit = before == (lane_id % cap).astype(jnp.float32)
        quarter = (lane_id // cap) % quarters
        block = source[slot].reshape(span, lanes)
        for q in range(quarters):
            here = hit & (quarter == q)
            picker = jnp.concatenate(
                [ones_where(named_0 & here), ones_where(named_1 & here)], axis=0
            )
            picked = dot32(picker, block)
            total[:, q * lanes : (q + 1) * lanes] += (
                picked[:rows] * weight_ref[:, 0:1] + picked[rows:] * weight_ref[:, 1:2]
            )

    combine(0, yr, own)

    def collect(slot, carry):
        b, h = slot // 2, slot % 2
        off = jnp.where(h == 0, b + 1, n_tp - 1 - b)
        wait_bytes(xr.at[slot], xr_sem.at[slot])
        combine(off, xr, slot)
        return carry

    lax.fori_loop(0, own, collect, 0)
    wait_bytes(xr.at[own + 1], xr_sem.at[own + 1])
    combine(half, xr, own + 1)
    expert_out[...] = total[...].astype(jnp.bfloat16)

    halo.wait_send()
    wait_bytes(xs.at[pl.ds(0, n_tp - 1)], xs_sem)
    wait_bytes(yd.at[:, pl.ds(0, n_ep - 1)], yf_sem)
    wait_bytes(ys.at[:, pl.ds(0, n_ep - 1)], ys_sem)
    wait_bytes(yr.at[pl.ds(0, n_tp - 1)], xb_sem)
    for step in range(1, half + 1):
        ring(step, 1).wait_send()
        if step < half:
            ring(step, -1).wait_send()


def on_device(
    pool_input,
    pool_map,
    pool_scale,
    out_weight,
    expert_input,
    norm_gain,
    routes,
    route_weight,
    gate_weight,
    up_weight,
    down_weight,
):
    n_ep, n_tp = lax.axis_size("ep"), lax.axis_size("tp")
    rows, width = expert_input.shape
    positions, channels = pool_input.shape
    hidden = gate_weight.shape[2]
    features = out_weight.shape[1]
    cap = 2 * rows * routes.shape[1] // (n_ep * n_tp)
    quarters = block_rows // cap
    lanes = width // quarters
    span = n_ep * block_rows
    half = n_tp // 2
    routes_t = jnp.pad(routes.T, ((0, 8 - routes.shape[1]), (0, 0)), constant_values=-1)
    vmem = pl.BlockSpec(memory_space=pltpu.VMEM)
    anywhere = pl.BlockSpec(memory_space=pl.ANY)
    bf16, f32 = jnp.bfloat16, jnp.float32
    exchange = pltpu.VMEM((n_tp, n_ep, block_rows, lanes), bf16)
    dma = pltpu.SemaphoreType.DMA
    return pl.pallas_call(
        functools.partial(kernel, n_ep, n_tp, cap),
        out_shape=(
            jax.ShapeDtypeStruct((positions, features), bf16),
            jax.ShapeDtypeStruct((rows, width), bf16),
        ),
        in_specs=[
            anywhere,
            vmem,
            vmem,
            vmem,
            vmem,
            anywhere,
            anywhere,
            anywhere,
            anywhere,
            anywhere,
            vmem,
            anywhere,
        ],
        out_specs=(vmem, vmem),
        scratch_shapes=[
            pltpu.VMEM((rows, width), bf16),
            pltpu.VMEM((width, hidden), bf16),
            pltpu.VMEM((width, hidden), bf16),
            pltpu.VMEM((hidden, width), bf16),
            pltpu.VMEM((positions, channels), bf16),
            pltpu.VMEM((channels, channels), bf16),
            pltpu.VMEM(out_weight.shape, bf16),
            pltpu.VMEM((halo_depth, channels), bf16),
            pltpu.VMEM((quarters * rows, lanes), bf16),
            exchange,
            exchange,
            exchange,
            exchange,
            exchange,
            exchange,
            pltpu.VMEM((2 * n_ep * cap, width), bf16),
            pltpu.VMEM((span, span), bf16),
            pltpu.VMEM((span, span), bf16),
            pltpu.VMEM((rows, width), f32),
            pltpu.VMEM((positions + halo_depth, channels), f32),
            pltpu.VMEM((3, positions + halo_depth, channels), f32),
            pltpu.VMEM((n_tp, positions, channels), bf16),
            dma((7,)),
            dma((2,)),
            dma,
            dma((n_tp,)),
            dma,
            dma((half,)),
            dma,
            dma((half,)),
            dma,
            dma((n_tp,)),
            dma((2, half)),
            dma((2, half)),
        ],
        compiler_params=pltpu.CompilerParams(
            collective_id=0, has_side_effects=True, vmem_limit_bytes=56 * 1024 * 1024
        ),
    )(
        expert_input,
        norm_gain.reshape(1, width),
        routes,
        routes_t,
        route_weight,
        gate_weight,
        up_weight,
        down_weight,
        pool_input,
        pool_map,
        pool_scale.reshape(n_tp, 1, channels),
        out_weight,
    )


def solution(mesh):
    return jax.shard_map(
        on_device,
        mesh=mesh,
        in_specs=(
            P(("grp", "ep"), "tp"),
            P(),
            P(),
            P(None, "tp"),
            P(("grp", "ep", "tp"), None),
            P(),
            P(("grp", "ep", "tp"), None),
            P(("grp", "ep", "tp"), None),
            P(("ep", "tp"), None, None),
            P(("ep", "tp"), None, None),
            P(("ep", "tp"), None, None),
        ),
        out_specs=(P(("grp", "ep"), "tp"), P(("grp", "ep", "tp"), None)),
        check_vma=False,
    )
```

```python
import functools

import jax
import jax.numpy as jnp
from jax import lax
from jax.experimental import pallas as pl
from jax.experimental.pallas import tpu as pltpu
from jax.sharding import PartitionSpec as P

MESH = pl.DeviceIdType.MESH
epsilon = 1e-06
halo_depth = 16
block_rows = 16
pairs = ((2, 6), (1, 7), (3, 5), (4, 0))
agenda = ("r0", "r1", "e0", "r2", "s1", "k0", "r3", "w1", "s2", "e2", "w2", "s3", "e3", "w3", "s4", "e1", "k2", "k3", "k1", "w4")


def dot32(a, b):
    return jnp.dot(a, b, preferred_element_type=jnp.float32)


def iota(shape, dim):
    return lax.broadcasted_iota(jnp.int32, shape, dim)


def ones_where(mask):
    return jnp.where(mask, 1.0, 0.0).astype(jnp.bfloat16)


def kernel(
    n_ep,
    n_tp,
    cap,
    x_hbm,
    gain_hbm,
    routes_hbm,
    weight_hbm,
    gate_hbm,
    up_hbm,
    down_hbm,
    pool_hbm,
    map_hbm,
    scale_hbm,
    proj_hbm,
    pool_out,
    expert_out,
    gain_ref,
    routes_ref,
    weight_ref,
    scale_ref,
    x_v,
    gate_v,
    up_v,
    down_v,
    pool_v,
    map_v,
    proj_v,
    halo_v,
    stacked,
    xs,
    xd,
    yd,
    ys,
    yr,
    xr,
    rows_v,
    perm,
    perm_t,
    total,
    ext,
    sums,
    gathered,
    local_sem,
    halo_sem,
    xs_sem,
    xd_sem,
    yf_sem,
    yd_sem,
    ys_sem,
    yr_sem,
    xb_sem,
    xr_sem,
    ring_send,
    ring_recv,
):
    ep = lax.axis_index("ep")
    tp = lax.axis_index("tp")
    half = n_tp // 2
    rows, width = x_v.shape
    quarters = block_rows // cap
    lanes = width // quarters
    span = n_ep * block_rows
    part = n_ep * cap

    own = [off for pair in pairs for off in pair].index(0)

    def offset(slot):
        return pairs[slot // 2][slot % 2]

    def twin(slot):
        return slot if slot // 2 == own // 2 else slot ^ 1

    barrier = pltpu.get_barrier_semaphore()
    for r in range(1, n_tp):
        pl.semaphore_signal(
            barrier, inc=1, device_id={"tp": lax.rem(tp + r, n_tp)}, device_id_type=MESH
        )

    def greet(r, carry):
        pl.semaphore_signal(
            barrier, inc=1, device_id={"ep": lax.rem(ep + r, n_ep)}, device_id_type=MESH
        )
        return carry

    lax.fori_loop(1, n_ep, greet, 0)

    moves = [
        (x_hbm, x_v),
        (gain_hbm, gain_ref),
        (routes_hbm, routes_ref),
        (pool_hbm, pool_v),
        (map_hbm.at[tp], map_v),
        (scale_hbm.at[tp], scale_ref),
        (gate_hbm.at[0], gate_v),
        (up_hbm.at[0], up_v),
        (down_hbm.at[0], down_v),
        (proj_hbm, proj_v),
        (weight_hbm, weight_ref),
    ]
    loads = [
        pltpu.make_async_copy(source, target, local_sem.at[n])
        for n, (source, target) in enumerate(moves)
    ]
    for load in loads:
        load.start()

    later = ones_where(iota((rows, rows), 0) < iota((rows, rows), 1))
    earlier = ones_where(iota((rows, rows), 0) > iota((rows, rows), 1))
    row_id, col_id = iota((span, span), 0), iota((span, span), 1)

    def home(v):
        return ((v // cap) % n_ep) * block_rows + (v // part) * cap + v % cap

    perm[...] = ones_where(home(row_id) == col_id)
    perm_t[...] = ones_where(row_id == home(col_id))

    for load in loads[:3]:
        load.wait()
    widened = x_v[...].astype(jnp.float32)
    normed = (
        widened
        * lax.rsqrt(jnp.mean(widened * widened, axis=1, keepdims=True) + epsilon)
        * gain_ref[...]
    ).astype(jnp.bfloat16)
    for q in range(quarters):
        stacked[q * rows : (q + 1) * rows, :] = normed[:, q * lanes : (q + 1) * lanes]

    slot_row = iota((span, rows), 0)

    def build(slot, off):
        expert = (slot_row // block_rows) * n_tp + lax.rem(tp + off, n_tp)
        named = (routes_ref[0:1, :] == expert) | (routes_ref[1:2, :] == expert)
        before = dot32(ones_where(named), later)
        chosen = named & (before == (slot_row % cap).astype(jnp.float32))
        quarter = (slot_row // cap) % quarters
        selector = jnp.concatenate(
            [ones_where(chosen & (quarter == q)) for q in range(quarters)], axis=1
        )
        block = dot32(selector, stacked[...]).astype(jnp.bfloat16)
        xs[slot] = block.reshape(n_ep, block_rows, lanes)

    def send_x(slot):
        pltpu.make_async_remote_copy(
            src_ref=xs.at[slot],
            dst_ref=xd.at[twin(slot)],
            send_sem=xs_sem,
            recv_sem=xd_sem.at[twin(slot)],
            device_id={"tp": lax.rem(tp + offset(slot), n_tp)},
            device_id_type=MESH,
        ).start()

    def forward_y(slot, source):
        def one(r, carry):
            peer = lax.rem(ep + r, n_ep)
            pltpu.make_async_remote_copy(
                src_ref=source.at[slot, peer],
                dst_ref=yd.at[slot, ep],
                send_sem=yf_sem,
                recv_sem=yd_sem.at[slot // 2],
                device_id={"ep": peer},
                device_id_type=MESH,
            ).start()
            return carry

        lax.fori_loop(1, n_ep, one, 0)
        yd[slot, ep] = source[slot, ep]

    def wait_bytes(ref, sem, name="drain"):
        with jax.named_scope(name):
            pltpu.make_async_copy(ref, ref, sem).wait()

    order = [slot for slot in range(n_tp) if slot != own]
    build(order[0], offset(order[0]))
    with jax.named_scope("barrier"):
        pl.semaphore_wait(barrier, n_tp - 1 + n_ep - 1)
    halo = pltpu.make_async_remote_copy(
        src_ref=pool_v.at[pool_v.shape[0] - halo_depth :],
        dst_ref=halo_v,
        send_sem=halo_sem.at[0],
        recv_sem=halo_sem.at[1],
        device_id={"ep": lax.rem(ep + 1, n_ep)},
        device_id_type=MESH,
    )
    build(order[1], offset(order[1]))
    send_x(order[0])
    build(own, 0)
    send_x(order[1])
    loads[3].wait()
    halo.start()
    build(order[2], offset(order[2]))
    forward_y(own, xs)
    for n in range(3, len(order)):
        build(order[n], offset(order[n]))
        send_x(order[n - 1])
    send_x(order[-1])

    for load in loads[4:6]:
        load.wait()
    positions, channels = pool_v.shape
    ext[halo_depth:, :] = pool_v[...].astype(jnp.float32)
    with jax.named_scope("halo"):
        halo.wait_recv()
    halo_rows = halo_v[...].astype(jnp.float32)
    ext[0:halo_depth, :] = jnp.where(ep == 0, jnp.zeros_like(halo_rows), halo_rows)
    level = lax.rem(tp, 4)
    summed = ext[halo_depth:, :] + ext[halo_depth - 1 : -1, :]
    sums[0, halo_depth:, :] = summed
    sums[0, 1:halo_depth, :] = ext[1:halo_depth, :] + ext[0 : halo_depth - 1, :]
    reach = 2
    first = 1
    for n in range(3):
        first = first + reach
        wider = sums[n, first:, :] + sums[n, first - reach : -reach, :]
        if n < 2:
            sums[n + 1, first:, :] = wider
        summed = jnp.where(level > n, wider[halo_depth - first :], summed)
        reach = 2 * reach
    window = jnp.left_shift(2, level)
    position = ep * positions + iota((positions, channels), 0)
    counted = jnp.minimum(position + 1, window).astype(jnp.float32)
    pooled = (summed / counted - ext[halo_depth:, :]).astype(jnp.bfloat16)
    mapped = dot32(pooled, map_v[...]) * scale_ref[...]
    gathered[tp] = mapped.astype(jnp.bfloat16)

    def ring(step, way):
        block = lax.rem(tp + n_tp - way * (step - 1), n_tp)
        lane = (1 - way) // 2
        return pltpu.make_async_remote_copy(
            src_ref=gathered.at[block],
            dst_ref=gathered.at[block],
            send_sem=ring_send.at[lane, step - 1],
            recv_sem=ring_recv.at[lane, step - 1],
            device_id={"tp": lax.rem(tp + n_tp + way, n_tp)},
            device_id_type=MESH,
        )

    def relay(b):
        for slot in (2 * b, 2 * b + 1):
            if slot != own:
                wait_bytes(xd.at[slot], xd_sem.at[slot], f"xd_{slot}")
                forward_y(slot, xd)

    def send_back(b):
        for slot in (2 * b, 2 * b + 1):
            wait_bytes(yr.at[slot, pl.ds(0, n_ep - 1)], yr_sem.at[slot], f"yr_{slot}")
            if slot != own:
                pltpu.make_async_remote_copy(
                    src_ref=yr.at[slot],
                    dst_ref=xr.at[twin(slot)],
                    send_sem=xb_sem,
                    recv_sem=xr_sem.at[twin(slot)],
                    device_id={"tp": lax.rem(tp + offset(slot), n_tp)},
                    device_id_type=MESH,
                ).start()

    def experts(b):
        wait_bytes(yd.at[pl.ds(2 * b, 2), pl.ds(0, n_ep - 1)], yd_sem.at[b], f"yd_{b}")
        for h in range(2):
            block = yd[2 * b + h].reshape(span, lanes)
            ordered = dot32(perm[...], block).astype(jnp.bfloat16)
            for q in range(quarters):
                rows_v[h * part : (h + 1) * part, q * lanes : (q + 1) * lanes] = ordered[
                    q * part : (q + 1) * part, :
                ]
        gate = dot32(rows_v[...], gate_v[...])
        up = dot32(rows_v[...], up_v[...])
        hidden = (gate / (1.0 + jnp.exp(-gate)) * up).astype(jnp.bfloat16)
        result = dot32(hidden, down_v[...]).astype(jnp.bfloat16)
        for h in range(2):
            tall = jnp.concatenate(
                [
                    result[h * part : (h + 1) * part, q * lanes : (q + 1) * lanes]
                    for q in range(quarters)
                ],
                axis=0,
            )
            block = dot32(perm_t[...], tall).astype(jnp.bfloat16)
            ys[2 * b + h] = block.reshape(n_ep, block_rows, lanes)
        for h in range(2):
            yr[2 * b + h, ep] = ys[2 * b + h, ep]

        def one(n, c):
            h = n // (n_ep - 1)
            peer = lax.rem(ep + 1 + n - h * (n_ep - 1), n_ep)
            pltpu.make_async_remote_copy(
                src_ref=ys.at[2 * b + h, peer],
                dst_ref=yr.at[2 * b + h, ep],
                send_sem=ys_sem,
                recv_sem=yr_sem.at[2 * b + h],
                device_id={"ep": peer},
                device_id_type=MESH,
            ).start()
            return c

        lax.fori_loop(0, 2 * (n_ep - 1), one, 0)

    def ring_start(step):
        ring(step, 1).start()
        if step < half:
            ring(step, -1).start()

    def ring_wait(step):
        with jax.named_scope(f"ring_{step}"):
            ring(step, 1).wait_recv()
            if step < half:
                ring(step, -1).wait_recv()

    for load in loads[6:]:
        load.wait()
    calls = {
        "r": relay,
        "e": experts,
        "k": send_back,
        "s": ring_start,
        "w": ring_wait,
    }
    for step in agenda:
        calls[step[0]](int(step[1]))

    tile = positions // 4

    def project(n, carry):
        at = pl.ds(pl.multiple_of(n * tile, tile), tile)
        left = jnp.concatenate([gathered[j, at, :] for j in range(n_tp)], axis=1)
        pool_out[at, :] = dot32(left, proj_v[...]).astype(jnp.bfloat16)
        return carry

    lax.fori_loop(0, 4, project, 0)

    total[...] = jnp.zeros_like(total)
    lane_id = iota((rows, span), 1)

    def upright(ref, k):
        return jnp.broadcast_to(ref[k : k + 1, :], (rows, rows)).T[:, 0:1]

    expert_0, expert_1 = upright(routes_ref, 0), upright(routes_ref, 1)
    weight_0, weight_1 = upright(weight_ref, 0), upright(weight_ref, 1)

    def combine(off, source, slot):
        expert = (lane_id // block_rows) * n_tp + lax.rem(tp + off, n_tp)
        named_0 = expert_0 == expert
        named_1 = expert_1 == expert
        before = dot32(earlier, ones_where(named_0 | named_1))
        hit = before == (lane_id % cap).astype(jnp.float32)
        quarter = (lane_id // cap) % quarters
        block = source[slot].reshape(span, lanes)
        for q in range(quarters):
            here = hit & (quarter == q)
            picker = jnp.concatenate(
                [ones_where(named_0 & here), ones_where(named_1 & here)], axis=0
            )
            picked = dot32(picker, block)
            total[:, q * lanes : (q + 1) * lanes] += (
                picked[:rows] * weight_0 + picked[rows:] * weight_1
            )

    combine(0, yr, own)
    for slot in order:
        wait_bytes(xr.at[slot], xr_sem.at[slot], f"xr_{slot}")
        combine(offset(slot), xr, slot)
    expert_out[...] = total[...].astype(jnp.bfloat16)

    halo.wait_send()
    wait_bytes(xs.at[pl.ds(0, n_tp - 1)], xs_sem)
    wait_bytes(yd.at[:, pl.ds(0, n_ep - 1)], yf_sem)
    wait_bytes(ys.at[:, pl.ds(0, n_ep - 1)], ys_sem)
    wait_bytes(yr.at[pl.ds(0, n_tp - 1)], xb_sem)
    for step in range(1, half + 1):
        ring(step, 1).wait_send()
        if step < half:
            ring(step, -1).wait_send()


def held(array):
    return pltpu.with_memory_space_constraint(array, pltpu.HBM)


def on_device(
    pool_input,
    pool_map,
    pool_scale,
    out_weight,
    expert_input,
    norm_gain,
    routes,
    route_weight,
    gate_weight,
    up_weight,
    down_weight,
):
    n_ep, n_tp = lax.axis_size("ep"), lax.axis_size("tp")
    rows, width = expert_input.shape
    positions, channels = pool_input.shape
    hidden = gate_weight.shape[2]
    features = out_weight.shape[1]
    cap = 2 * rows * routes.shape[1] // (n_ep * n_tp)
    quarters = block_rows // cap
    lanes = width // quarters
    span = n_ep * block_rows
    half = n_tp // 2
    vmem = pl.BlockSpec(memory_space=pltpu.VMEM)
    far = pl.BlockSpec(memory_space=pl.ANY)
    bf16, f32 = jnp.bfloat16, jnp.float32
    exchange = pltpu.VMEM((n_tp, n_ep, block_rows, lanes), bf16)
    dma = pltpu.SemaphoreType.DMA
    return pl.pallas_call(
        functools.partial(kernel, n_ep, n_tp, cap),
        out_shape=(
            jax.ShapeDtypeStruct((positions, features), bf16),
            jax.ShapeDtypeStruct((rows, width), bf16),
        ),
        in_specs=[far] * 11,
        out_specs=(vmem, vmem),
        scratch_shapes=[
            pltpu.VMEM((1, width), f32),
            pltpu.VMEM(routes.T.shape, jnp.int32),
            pltpu.VMEM(routes.T.shape, f32),
            pltpu.VMEM((1, channels), f32),
            pltpu.VMEM((rows, width), bf16),
            pltpu.VMEM((width, hidden), bf16),
            pltpu.VMEM((width, hidden), bf16),
            pltpu.VMEM((hidden, width), bf16),
            pltpu.VMEM((positions, channels), bf16),
            pltpu.VMEM((channels, channels), bf16),
            pltpu.VMEM(out_weight.shape, bf16),
            pltpu.VMEM((halo_depth, channels), bf16),
            pltpu.VMEM((quarters * rows, lanes), bf16),
            exchange,
            exchange,
            exchange,
            exchange,
            exchange,
            exchange,
            pltpu.VMEM((2 * n_ep * cap, width), bf16),
            pltpu.VMEM((span, span), bf16),
            pltpu.VMEM((span, span), bf16),
            pltpu.VMEM((rows, width), f32),
            pltpu.VMEM((positions + halo_depth, channels), f32),
            pltpu.VMEM((3, positions + halo_depth, channels), f32),
            pltpu.VMEM((n_tp, positions, channels), bf16),
            dma((11,)),
            dma((2,)),
            dma,
            dma((n_tp,)),
            dma,
            dma((half,)),
            dma,
            dma((n_tp,)),
            dma,
            dma((n_tp,)),
            dma((2, half)),
            dma((2, half)),
        ],
        compiler_params=pltpu.CompilerParams(
            collective_id=0, has_side_effects=True, vmem_limit_bytes=50 * 1024 * 1024
        ),
    )(
        *map(
            held,
            (
                expert_input,
                norm_gain.reshape(1, width),
                routes.T,
                route_weight.T,
                gate_weight,
                up_weight,
                down_weight,
                pool_input,
                pool_map,
                pool_scale.reshape(n_tp, 1, channels),
                out_weight,
            ),
        )
    )


def solution(mesh):
    return jax.shard_map(
        on_device,
        mesh=mesh,
        in_specs=(
            P(("grp", "ep"), "tp"),
            P(),
            P(),
            P(None, "tp"),
            P(("grp", "ep", "tp"), None),
            P(),
            P(("grp", "ep", "tp"), None),
            P(("grp", "ep", "tp"), None),
            P(("ep", "tp"), None, None),
            P(("ep", "tp"), None, None),
            P(("ep", "tp"), None, None),
        ),
        out_specs=(P(("grp", "ep"), "tp"), P(("grp", "ep", "tp"), None)),
        check_vma=False,
    )
```

```python
import functools

import jax
import jax.numpy as jnp
from jax import lax
from jax.experimental import pallas as pl
from jax.experimental.pallas import tpu as pltpu
from jax.sharding import PartitionSpec as P

MESH = pl.DeviceIdType.MESH
epsilon = 1e-06
halo_depth = 16
block_rows = 16
pairs = ((2, 6), (1, 7), (3, 5), (4, 0))
agenda = ("r0", "r1", "e0", "r2", "s1", "k0", "r3", "w1", "s2", "e2", "w2", "s3", "e3", "k2", "w3", "s4", "e1", "k3", "k1", "w4")


def dot32(a, b):
    return jnp.dot(a, b, preferred_element_type=jnp.float32)


def iota(shape, dim):
    return lax.broadcasted_iota(jnp.int32, shape, dim)


def ones_where(mask):
    return jnp.where(mask, 1.0, 0.0).astype(jnp.bfloat16)


def kernel(
    n_ep,
    n_tp,
    cap,
    x_hbm,
    gain_hbm,
    routes_hbm,
    weight_hbm,
    gate_hbm,
    up_hbm,
    down_hbm,
    pool_hbm,
    map_hbm,
    scale_hbm,
    proj_hbm,
    pool_out,
    expert_out,
    gain_ref,
    routes_ref,
    weight_ref,
    scale_ref,
    x_v,
    gate_v,
    up_v,
    down_v,
    pool_v,
    map_v,
    proj_v,
    halo_v,
    stacked,
    xs,
    xd,
    yd,
    ys,
    yr,
    xr,
    rows_v,
    perm,
    perm_t,
    total,
    ext,
    sums,
    gathered,
    local_sem,
    halo_sem,
    xs_sem,
    xd_sem,
    yf_sem,
    yd_sem,
    ys_sem,
    yr_sem,
    xb_sem,
    xr_sem,
    ring_send,
    ring_recv,
):
    ep = lax.axis_index("ep")
    tp = lax.axis_index("tp")
    half = n_tp // 2
    rows, width = x_v.shape
    quarters = block_rows // cap
    lanes = width // quarters
    span = n_ep * block_rows
    part = n_ep * cap

    own = [off for pair in pairs for off in pair].index(0)

    def offset(slot):
        return pairs[slot // 2][slot % 2]

    def twin(slot):
        return slot if slot // 2 == own // 2 else slot ^ 1

    barrier = pltpu.get_barrier_semaphore()
    for r in range(1, n_tp):
        pl.semaphore_signal(
            barrier, inc=1, device_id={"tp": lax.rem(tp + r, n_tp)}, device_id_type=MESH
        )

    def greet(r, carry):
        pl.semaphore_signal(
            barrier, inc=1, device_id={"ep": lax.rem(ep + r, n_ep)}, device_id_type=MESH
        )
        return carry

    lax.fori_loop(1, n_ep, greet, 0)

    moves = [
        (x_hbm, x_v),
        (gain_hbm, gain_ref),
        (routes_hbm, routes_ref),
        (pool_hbm, pool_v),
        (map_hbm.at[tp], map_v),
        (scale_hbm.at[tp], scale_ref),
        (gate_hbm.at[0], gate_v),
        (up_hbm.at[0], up_v),
        (down_hbm.at[0], down_v),
        (proj_hbm, proj_v),
        (weight_hbm, weight_ref),
    ]
    loads = [
        pltpu.make_async_copy(source, target, local_sem.at[n])
        for n, (source, target) in enumerate(moves)
    ]
    for load in loads:
        load.start()

    later = ones_where(iota((rows, rows), 0) < iota((rows, rows), 1))
    earlier = ones_where(iota((rows, rows), 0) > iota((rows, rows), 1))
    row_id, col_id = iota((span, span), 0), iota((span, span), 1)

    def home(v):
        return ((v // cap) % n_ep) * block_rows + (v // part) * cap + v % cap

    perm[...] = ones_where(home(row_id) == col_id)
    perm_t[...] = ones_where(row_id == home(col_id))

    for load in loads[:3]:
        load.wait()
    widened = x_v[...].astype(jnp.float32)
    normed = (
        widened
        * lax.rsqrt(jnp.mean(widened * widened, axis=1, keepdims=True) + epsilon)
        * gain_ref[...]
    ).astype(jnp.bfloat16)
    for q in range(quarters):
        stacked[q * rows : (q + 1) * rows, :] = normed[:, q * lanes : (q + 1) * lanes]

    slot_row = iota((span, rows), 0)

    def build(slot, off):
        expert = (slot_row // block_rows) * n_tp + lax.rem(tp + off, n_tp)
        named = (routes_ref[0:1, :] == expert) | (routes_ref[1:2, :] == expert)
        before = dot32(ones_where(named), later)
        chosen = named & (before == (slot_row % cap).astype(jnp.float32))
        quarter = (slot_row // cap) % quarters
        selector = jnp.concatenate(
            [ones_where(chosen & (quarter == q)) for q in range(quarters)], axis=1
        )
        block = dot32(selector, stacked[...]).astype(jnp.bfloat16)
        xs[slot] = block.reshape(n_ep, block_rows, lanes)

    def send_x(slot):
        pltpu.make_async_remote_copy(
            src_ref=xs.at[slot],
            dst_ref=xd.at[twin(slot)],
            send_sem=xs_sem,
            recv_sem=xd_sem.at[twin(slot)],
            device_id={"tp": lax.rem(tp + offset(slot), n_tp)},
            device_id_type=MESH,
        ).start()

    def forward_y(slot, source):
        def one(r, carry):
            peer = lax.rem(ep + r, n_ep)
            pltpu.make_async_remote_copy(
                src_ref=source.at[slot, peer],
                dst_ref=yd.at[slot, ep],
                send_sem=yf_sem,
                recv_sem=yd_sem.at[slot // 2],
                device_id={"ep": peer},
                device_id_type=MESH,
            ).start()
            return carry

        lax.fori_loop(1, n_ep, one, 0)
        yd[slot, ep] = source[slot, ep]

    def wait_bytes(ref, sem, name="drain"):
        with jax.named_scope(name):
            pltpu.make_async_copy(ref, ref, sem).wait()

    order = [slot for slot in range(n_tp) if slot != own]
    build(order[0], offset(order[0]))
    with jax.named_scope("barrier"):
        pl.semaphore_wait(barrier, n_tp - 1 + n_ep - 1)
    halo = pltpu.make_async_remote_copy(
        src_ref=pool_v.at[pool_v.shape[0] - halo_depth :],
        dst_ref=halo_v,
        send_sem=halo_sem.at[0],
        recv_sem=halo_sem.at[1],
        device_id={"ep": lax.rem(ep + 1, n_ep)},
        device_id_type=MESH,
    )
    build(order[1], offset(order[1]))
    send_x(order[0])
    build(own, 0)
    send_x(order[1])
    loads[3].wait()
    halo.start()
    build(order[2], offset(order[2]))
    forward_y(own, xs)
    for n in range(3, len(order)):
        build(order[n], offset(order[n]))
        send_x(order[n - 1])
    send_x(order[-1])

    for load in loads[4:6]:
        load.wait()
    positions, channels = pool_v.shape
    ext[halo_depth:, :] = pool_v[...].astype(jnp.float32)
    with jax.named_scope("halo"):
        halo.wait_recv()
    halo_rows = halo_v[...].astype(jnp.float32)
    ext[0:halo_depth, :] = jnp.where(ep == 0, jnp.zeros_like(halo_rows), halo_rows)
    level = lax.rem(tp, 4)
    summed = ext[halo_depth:, :] + ext[halo_depth - 1 : -1, :]
    sums[0, halo_depth:, :] = summed
    sums[0, 1:halo_depth, :] = ext[1:halo_depth, :] + ext[0 : halo_depth - 1, :]
    reach = 2
    first = 1
    for n in range(3):
        first = first + reach
        wider = sums[n, first:, :] + sums[n, first - reach : -reach, :]
        if n < 2:
            sums[n + 1, first:, :] = wider
        summed = jnp.where(level > n, wider[halo_depth - first :], summed)
        reach = 2 * reach
    window = jnp.left_shift(2, level)
    position = ep * positions + iota((positions, channels), 0)
    counted = jnp.minimum(position + 1, window).astype(jnp.float32)
    pooled = (summed / counted - ext[halo_depth:, :]).astype(jnp.bfloat16)
    mapped = dot32(pooled, map_v[...]) * scale_ref[...]
    gathered[tp] = mapped.astype(jnp.bfloat16)

    def ring(step, way):
        block = lax.rem(tp + n_tp - way * (step - 1), n_tp)
        lane = (1 - way) // 2
        return pltpu.make_async_remote_copy(
            src_ref=gathered.at[block],
            dst_ref=gathered.at[block],
            send_sem=ring_send.at[lane, step - 1],
            recv_sem=ring_recv.at[lane, step - 1],
            device_id={"tp": lax.rem(tp + n_tp + way, n_tp)},
            device_id_type=MESH,
        )

    def relay(b):
        for slot in (2 * b, 2 * b + 1):
            if slot != own:
                wait_bytes(xd.at[slot], xd_sem.at[slot], f"xd_{slot}")
                forward_y(slot, xd)

    def send_back(b):
        for slot in (2 * b, 2 * b + 1):
            wait_bytes(yr.at[slot, pl.ds(0, n_ep - 1)], yr_sem.at[slot], f"yr_{slot}")
            if slot != own:
                pltpu.make_async_remote_copy(
                    src_ref=yr.at[slot],
                    dst_ref=xr.at[twin(slot)],
                    send_sem=xb_sem,
                    recv_sem=xr_sem.at[twin(slot)],
                    device_id={"tp": lax.rem(tp + offset(slot), n_tp)},
                    device_id_type=MESH,
                ).start()

    def experts(b):
        wait_bytes(yd.at[pl.ds(2 * b, 2), pl.ds(0, n_ep - 1)], yd_sem.at[b], f"yd_{b}")
        for h in range(2):
            block = yd[2 * b + h].reshape(span, lanes)
            ordered = dot32(perm[...], block).astype(jnp.bfloat16)
            for q in range(quarters):
                rows_v[h * part : (h + 1) * part, q * lanes : (q + 1) * lanes] = ordered[
                    q * part : (q + 1) * part, :
                ]
        gate = dot32(rows_v[...], gate_v[...])
        up = dot32(rows_v[...], up_v[...])
        hidden = (gate / (1.0 + jnp.exp(-gate)) * up).astype(jnp.bfloat16)
        result = dot32(hidden, down_v[...]).astype(jnp.bfloat16)
        for h in range(2):
            tall = jnp.concatenate(
                [
                    result[h * part : (h + 1) * part, q * lanes : (q + 1) * lanes]
                    for q in range(quarters)
                ],
                axis=0,
            )
            block = dot32(perm_t[...], tall).astype(jnp.bfloat16)
            ys[2 * b + h] = block.reshape(n_ep, block_rows, lanes)
        for h in range(2):
            yr[2 * b + h, ep] = ys[2 * b + h, ep]

        def one(n, c):
            h = n // (n_ep - 1)
            peer = lax.rem(ep + 1 + n - h * (n_ep - 1), n_ep)
            pltpu.make_async_remote_copy(
                src_ref=ys.at[2 * b + h, peer],
                dst_ref=yr.at[2 * b + h, ep],
                send_sem=ys_sem,
                recv_sem=yr_sem.at[2 * b + h],
                device_id={"ep": peer},
                device_id_type=MESH,
            ).start()
            return c

        lax.fori_loop(0, 2 * (n_ep - 1), one, 0)

    def ring_start(step):
        ring(step, 1).start()
        if step < half:
            ring(step, -1).start()

    def ring_wait(step):
        with jax.named_scope(f"ring_{step}"):
            ring(step, 1).wait_recv()
            if step < half:
                ring(step, -1).wait_recv()

    for load in loads[6:]:
        load.wait()
    calls = {
        "r": relay,
        "e": experts,
        "k": send_back,
        "s": ring_start,
        "w": ring_wait,
    }
    for step in agenda:
        calls[step[0]](int(step[1]))

    tile = positions // 4

    def project(n, carry):
        at = pl.ds(pl.multiple_of(n * tile, tile), tile)
        left = jnp.concatenate([gathered[j, at, :] for j in range(n_tp)], axis=1)
        pool_out[at, :] = dot32(left, proj_v[...]).astype(jnp.bfloat16)
        return carry

    lax.fori_loop(0, 4, project, 0)

    total[...] = jnp.zeros_like(total)
    lane_id = iota((rows, span), 1)

    def upright(ref, k):
        return jnp.broadcast_to(ref[k : k + 1, :], (rows, rows)).T[:, 0:1]

    expert_0, expert_1 = upright(routes_ref, 0), upright(routes_ref, 1)
    weight_0, weight_1 = upright(weight_ref, 0), upright(weight_ref, 1)

    def combine(off, source, slot):
        expert = (lane_id // block_rows) * n_tp + lax.rem(tp + off, n_tp)
        named_0 = expert_0 == expert
        named_1 = expert_1 == expert
        before = dot32(earlier, ones_where(named_0 | named_1))
        hit = before == (lane_id % cap).astype(jnp.float32)
        quarter = (lane_id // cap) % quarters
        block = source[slot].reshape(span, lanes)
        for q in range(quarters):
            here = hit & (quarter == q)
            picker = jnp.concatenate(
                [ones_where(named_0 & here), ones_where(named_1 & here)], axis=0
            )
            picked = dot32(picker, block)
            total[:, q * lanes : (q + 1) * lanes] += (
                picked[:rows] * weight_0 + picked[rows:] * weight_1
            )

    combine(0, yr, own)
    arrival = [2 * int(step[1]) + h for step in agenda if step[0] == "k" for h in range(2)]
    for slot in arrival:
        if slot == own:
            continue
        wait_bytes(xr.at[slot], xr_sem.at[slot], f"xr_{slot}")
        combine(offset(slot), xr, slot)
    expert_out[...] = total[...].astype(jnp.bfloat16)

    halo.wait_send()
    wait_bytes(xs.at[pl.ds(0, n_tp - 1)], xs_sem)
    wait_bytes(yd.at[:, pl.ds(0, n_ep - 1)], yf_sem)
    wait_bytes(ys.at[:, pl.ds(0, n_ep - 1)], ys_sem)
    wait_bytes(yr.at[pl.ds(0, n_tp - 1)], xb_sem)
    for step in range(1, half + 1):
        ring(step, 1).wait_send()
        if step < half:
            ring(step, -1).wait_send()


def held(array):
    return pltpu.with_memory_space_constraint(array, pltpu.HBM)


def on_device(
    pool_input,
    pool_map,
    pool_scale,
    out_weight,
    expert_input,
    norm_gain,
    routes,
    route_weight,
    gate_weight,
    up_weight,
    down_weight,
):
    n_ep, n_tp = lax.axis_size("ep"), lax.axis_size("tp")
    rows, width = expert_input.shape
    positions, channels = pool_input.shape
    hidden = gate_weight.shape[2]
    features = out_weight.shape[1]
    cap = 2 * rows * routes.shape[1] // (n_ep * n_tp)
    quarters = block_rows // cap
    lanes = width // quarters
    span = n_ep * block_rows
    half = n_tp // 2
    vmem = pl.BlockSpec(memory_space=pltpu.VMEM)
    far = pl.BlockSpec(memory_space=pl.ANY)
    bf16, f32 = jnp.bfloat16, jnp.float32
    exchange = pltpu.VMEM((n_tp, n_ep, block_rows, lanes), bf16)
    dma = pltpu.SemaphoreType.DMA
    return pl.pallas_call(
        functools.partial(kernel, n_ep, n_tp, cap),
        out_shape=(
            jax.ShapeDtypeStruct((positions, features), bf16),
            jax.ShapeDtypeStruct((rows, width), bf16),
        ),
        in_specs=[far] * 11,
        out_specs=(vmem, vmem),
        scratch_shapes=[
            pltpu.VMEM((1, width), f32),
            pltpu.VMEM(routes.T.shape, jnp.int32),
            pltpu.VMEM(routes.T.shape, f32),
            pltpu.VMEM((1, channels), f32),
            pltpu.VMEM((rows, width), bf16),
            pltpu.VMEM((width, hidden), bf16),
            pltpu.VMEM((width, hidden), bf16),
            pltpu.VMEM((hidden, width), bf16),
            pltpu.VMEM((positions, channels), bf16),
            pltpu.VMEM((channels, channels), bf16),
            pltpu.VMEM(out_weight.shape, bf16),
            pltpu.VMEM((halo_depth, channels), bf16),
            pltpu.VMEM((quarters * rows, lanes), bf16),
            exchange,
            exchange,
            exchange,
            exchange,
            exchange,
            exchange,
            pltpu.VMEM((2 * n_ep * cap, width), bf16),
            pltpu.VMEM((span, span), bf16),
            pltpu.VMEM((span, span), bf16),
            pltpu.VMEM((rows, width), f32),
            pltpu.VMEM((positions + halo_depth, channels), f32),
            pltpu.VMEM((3, positions + halo_depth, channels), f32),
            pltpu.VMEM((n_tp, positions, channels), bf16),
            dma((11,)),
            dma((2,)),
            dma,
            dma((n_tp,)),
            dma,
            dma((half,)),
            dma,
            dma((n_tp,)),
            dma,
            dma((n_tp,)),
            dma((2, half)),
            dma((2, half)),
        ],
        compiler_params=pltpu.CompilerParams(
            collective_id=0, has_side_effects=True, vmem_limit_bytes=50 * 1024 * 1024
        ),
    )(
        *map(
            held,
            (
                expert_input,
                norm_gain.reshape(1, width),
                routes.T,
                route_weight.T,
                gate_weight,
                up_weight,
                down_weight,
                pool_input,
                pool_map,
                pool_scale.reshape(n_tp, 1, channels),
                out_weight,
            ),
        )
    )


def solution(mesh):
    return jax.shard_map(
        on_device,
        mesh=mesh,
        in_specs=(
            P(("grp", "ep"), "tp"),
            P(),
            P(),
            P(None, "tp"),
            P(("grp", "ep", "tp"), None),
            P(),
            P(("grp", "ep", "tp"), None),
            P(("grp", "ep", "tp"), None),
            P(("ep", "tp"), None, None),
            P(("ep", "tp"), None, None),
            P(("ep", "tp"), None, None),
        ),
        out_specs=(P(("grp", "ep"), "tp"), P(("grp", "ep", "tp"), None)),
        check_vma=False,
    )
```

```python
import functools

import jax
import jax.numpy as jnp
from jax import lax
from jax.experimental import pallas as pl
from jax.experimental.pallas import tpu as pltpu
from jax.sharding import PartitionSpec as P

MESH = pl.DeviceIdType.MESH
epsilon = 1e-06
halo_depth = 16
block_rows = 16
pairs = ((2, 6), (1, 7), (3, 5), (4, 0))
agenda = ("r0", "r1", "e0", "s1", "r2", "w1", "s2", "k0", "r3", "e2", "w2", "s3", "e3", "k2", "w3", "s4", "e1", "k3", "k1", "w4")


def dot32(a, b):
    return jnp.dot(a, b, preferred_element_type=jnp.float32)


def iota(shape, dim):
    return lax.broadcasted_iota(jnp.int32, shape, dim)


def ones_where(mask):
    return jnp.where(mask, 1.0, 0.0).astype(jnp.bfloat16)


def kernel(
    n_ep,
    n_tp,
    cap,
    x_hbm,
    gain_hbm,
    routes_hbm,
    weight_hbm,
    gate_hbm,
    up_hbm,
    down_hbm,
    pool_hbm,
    map_hbm,
    scale_hbm,
    proj_hbm,
    pool_out,
    expert_out,
    gain_ref,
    routes_ref,
    weight_ref,
    scale_ref,
    x_v,
    gate_v,
    up_v,
    down_v,
    pool_v,
    map_v,
    proj_v,
    halo_v,
    stacked,
    xs,
    xd,
    yd,
    ys,
    yr,
    xr,
    rows_v,
    perm,
    perm_t,
    total,
    ext,
    sums,
    gathered,
    local_sem,
    halo_sem,
    xs_sem,
    xd_sem,
    yf_sem,
    yd_sem,
    ys_sem,
    yr_sem,
    xb_sem,
    xr_sem,
    ring_send,
    ring_recv,
):
    ep = lax.axis_index("ep")
    tp = lax.axis_index("tp")
    half = n_tp // 2
    rows, width = x_v.shape
    quarters = block_rows // cap
    lanes = width // quarters
    span = n_ep * block_rows
    part = n_ep * cap

    own = [off for pair in pairs for off in pair].index(0)

    def offset(slot):
        return pairs[slot // 2][slot % 2]

    def twin(slot):
        return slot if slot // 2 == own // 2 else slot ^ 1

    barrier = pltpu.get_barrier_semaphore()
    for r in range(1, n_tp):
        pl.semaphore_signal(
            barrier, inc=1, device_id={"tp": lax.rem(tp + r, n_tp)}, device_id_type=MESH
        )

    def greet(r, carry):
        pl.semaphore_signal(
            barrier, inc=1, device_id={"ep": lax.rem(ep + r, n_ep)}, device_id_type=MESH
        )
        return carry

    lax.fori_loop(1, n_ep, greet, 0)

    moves = [
        (x_hbm, x_v),
        (gain_hbm, gain_ref),
        (routes_hbm, routes_ref),
        (pool_hbm, pool_v),
        (map_hbm.at[tp], map_v),
        (scale_hbm.at[tp], scale_ref),
        (gate_hbm.at[0], gate_v),
        (up_hbm.at[0], up_v),
        (down_hbm.at[0], down_v),
        (proj_hbm, proj_v),
        (weight_hbm, weight_ref),
    ]
    loads = [
        pltpu.make_async_copy(source, target, local_sem.at[n])
        for n, (source, target) in enumerate(moves)
    ]
    for load in loads:
        load.start()

    later = ones_where(iota((rows, rows), 0) < iota((rows, rows), 1))
    earlier = ones_where(iota((rows, rows), 0) > iota((rows, rows), 1))
    row_id, col_id = iota((span, span), 0), iota((span, span), 1)

    def home(v):
        return ((v // cap) % n_ep) * block_rows + (v // part) * cap + v % cap

    perm[...] = ones_where(home(row_id) == col_id)
    perm_t[...] = ones_where(row_id == home(col_id))

    for load in loads[:3]:
        load.wait()
    widened = x_v[...].astype(jnp.float32)
    normed = (
        widened
        * lax.rsqrt(jnp.mean(widened * widened, axis=1, keepdims=True) + epsilon)
        * gain_ref[...]
    ).astype(jnp.bfloat16)
    for q in range(quarters):
        stacked[q * rows : (q + 1) * rows, :] = normed[:, q * lanes : (q + 1) * lanes]

    slot_row = iota((span, rows), 0)

    def build(slot, off):
        expert = (slot_row // block_rows) * n_tp + lax.rem(tp + off, n_tp)
        named = (routes_ref[0:1, :] == expert) | (routes_ref[1:2, :] == expert)
        before = dot32(ones_where(named), later)
        chosen = named & (before == (slot_row % cap).astype(jnp.float32))
        quarter = (slot_row // cap) % quarters
        selector = jnp.concatenate(
            [ones_where(chosen & (quarter == q)) for q in range(quarters)], axis=1
        )
        block = dot32(selector, stacked[...]).astype(jnp.bfloat16)
        xs[slot] = block.reshape(n_ep, block_rows, lanes)

    def send_x(slot):
        pltpu.make_async_remote_copy(
            src_ref=xs.at[slot],
            dst_ref=xd.at[twin(slot)],
            send_sem=xs_sem,
            recv_sem=xd_sem.at[twin(slot)],
            device_id={"tp": lax.rem(tp + offset(slot), n_tp)},
            device_id_type=MESH,
        ).start()

    def forward_y(slot, source):
        def one(r, carry):
            peer = lax.rem(ep + r, n_ep)
            pltpu.make_async_remote_copy(
                src_ref=source.at[slot, peer],
                dst_ref=yd.at[slot, ep],
                send_sem=yf_sem,
                recv_sem=yd_sem.at[slot // 2],
                device_id={"ep": peer},
                device_id_type=MESH,
            ).start()
            return carry

        lax.fori_loop(1, n_ep, one, 0)
        yd[slot, ep] = source[slot, ep]

    def wait_bytes(ref, sem, name="drain"):
        with jax.named_scope(name):
            pltpu.make_async_copy(ref, ref, sem).wait()

    order = [slot for slot in range(n_tp) if slot != own]
    build(order[0], offset(order[0]))
    with jax.named_scope("barrier"):
        pl.semaphore_wait(barrier, n_tp - 1 + n_ep - 1)
    halo = pltpu.make_async_remote_copy(
        src_ref=pool_v.at[pool_v.shape[0] - halo_depth :],
        dst_ref=halo_v,
        send_sem=halo_sem.at[0],
        recv_sem=halo_sem.at[1],
        device_id={"ep": lax.rem(ep + 1, n_ep)},
        device_id_type=MESH,
    )
    build(order[1], offset(order[1]))
    send_x(order[0])
    build(own, 0)
    send_x(order[1])
    loads[3].wait()
    halo.start()
    build(order[2], offset(order[2]))
    forward_y(own, xs)
    for n in range(3, len(order)):
        build(order[n], offset(order[n]))
        send_x(order[n - 1])
    send_x(order[-1])

    for load in loads[4:6]:
        load.wait()
    positions, channels = pool_v.shape
    ext[halo_depth:, :] = pool_v[...].astype(jnp.float32)
    with jax.named_scope("halo"):
        halo.wait_recv()
    halo_rows = halo_v[...].astype(jnp.float32)
    ext[0:halo_depth, :] = jnp.where(ep == 0, jnp.zeros_like(halo_rows), halo_rows)
    level = lax.rem(tp, 4)
    summed = ext[halo_depth:, :] + ext[halo_depth - 1 : -1, :]
    sums[0, halo_depth:, :] = summed
    sums[0, 1:halo_depth, :] = ext[1:halo_depth, :] + ext[0 : halo_depth - 1, :]
    reach = 2
    first = 1
    for n in range(3):
        first = first + reach
        wider = sums[n, first:, :] + sums[n, first - reach : -reach, :]
        if n < 2:
            sums[n + 1, first:, :] = wider
        summed = jnp.where(level > n, wider[halo_depth - first :], summed)
        reach = 2 * reach
    window = jnp.left_shift(2, level)
    position = ep * positions + iota((positions, channels), 0)
    counted = jnp.minimum(position + 1, window).astype(jnp.float32)
    pooled = (summed / counted - ext[halo_depth:, :]).astype(jnp.bfloat16)
    mapped = dot32(pooled, map_v[...]) * scale_ref[...]
    gathered[tp] = mapped.astype(jnp.bfloat16)

    def ring(step, way):
        block = lax.rem(tp + n_tp - way * (step - 1), n_tp)
        lane = (1 - way) // 2
        return pltpu.make_async_remote_copy(
            src_ref=gathered.at[block],
            dst_ref=gathered.at[block],
            send_sem=ring_send.at[lane, step - 1],
            recv_sem=ring_recv.at[lane, step - 1],
            device_id={"tp": lax.rem(tp + n_tp + way, n_tp)},
            device_id_type=MESH,
        )

    def relay(b):
        for slot in (2 * b, 2 * b + 1):
            if slot != own:
                wait_bytes(xd.at[slot], xd_sem.at[slot], f"xd_{slot}")
                forward_y(slot, xd)

    def send_back(b):
        for slot in (2 * b, 2 * b + 1):
            wait_bytes(yr.at[slot, pl.ds(0, n_ep - 1)], yr_sem.at[slot], f"yr_{slot}")
            if slot != own:
                pltpu.make_async_remote_copy(
                    src_ref=yr.at[slot],
                    dst_ref=xr.at[twin(slot)],
                    send_sem=xb_sem,
                    recv_sem=xr_sem.at[twin(slot)],
                    device_id={"tp": lax.rem(tp + offset(slot), n_tp)},
                    device_id_type=MESH,
                ).start()

    def experts(b):
        wait_bytes(yd.at[pl.ds(2 * b, 2), pl.ds(0, n_ep - 1)], yd_sem.at[b], f"yd_{b}")
        for h in range(2):
            block = yd[2 * b + h].reshape(span, lanes)
            ordered = dot32(perm[...], block).astype(jnp.bfloat16)
            for q in range(quarters):
                rows_v[h * part : (h + 1) * part, q * lanes : (q + 1) * lanes] = ordered[
                    q * part : (q + 1) * part, :
                ]
        gate = dot32(rows_v[...], gate_v[...])
        up = dot32(rows_v[...], up_v[...])
        hidden = (gate / (1.0 + jnp.exp(-gate)) * up).astype(jnp.bfloat16)
        result = dot32(hidden, down_v[...]).astype(jnp.bfloat16)
        for h in range(2):
            tall = jnp.concatenate(
                [
                    result[h * part : (h + 1) * part, q * lanes : (q + 1) * lanes]
                    for q in range(quarters)
                ],
                axis=0,
            )
            block = dot32(perm_t[...], tall).astype(jnp.bfloat16)
            ys[2 * b + h] = block.reshape(n_ep, block_rows, lanes)
        for h in range(2):
            yr[2 * b + h, ep] = ys[2 * b + h, ep]

        def one(n, c):
            h = n // (n_ep - 1)
            peer = lax.rem(ep + 1 + n - h * (n_ep - 1), n_ep)
            pltpu.make_async_remote_copy(
                src_ref=ys.at[2 * b + h, peer],
                dst_ref=yr.at[2 * b + h, ep],
                send_sem=ys_sem,
                recv_sem=yr_sem.at[2 * b + h],
                device_id={"ep": peer},
                device_id_type=MESH,
            ).start()
            return c

        lax.fori_loop(0, 2 * (n_ep - 1), one, 0)

    def ring_start(step):
        ring(step, 1).start()
        if step < half:
            ring(step, -1).start()

    def ring_wait(step):
        with jax.named_scope(f"ring_{step}"):
            ring(step, 1).wait_recv()
            if step < half:
                ring(step, -1).wait_recv()

    for load in loads[6:]:
        load.wait()
    calls = {
        "r": relay,
        "e": experts,
        "k": send_back,
        "s": ring_start,
        "w": ring_wait,
    }
    for step in agenda:
        calls[step[0]](int(step[1]))

    tile = positions // 4

    def project(n, carry):
        at = pl.ds(pl.multiple_of(n * tile, tile), tile)
        left = jnp.concatenate([gathered[j, at, :] for j in range(n_tp)], axis=1)
        pool_out[at, :] = dot32(left, proj_v[...]).astype(jnp.bfloat16)
        return carry

    lax.fori_loop(0, 4, project, 0)

    total[...] = jnp.zeros_like(total)
    lane_id = iota((rows, span), 1)

    def upright(ref, k):
        return jnp.broadcast_to(ref[k : k + 1, :], (rows, rows)).T[:, 0:1]

    expert_0, expert_1 = upright(routes_ref, 0), upright(routes_ref, 1)
    weight_0, weight_1 = upright(weight_ref, 0), upright(weight_ref, 1)

    def combine(off, source, slot):
        expert = (lane_id // block_rows) * n_tp + lax.rem(tp + off, n_tp)
        named_0 = expert_0 == expert
        named_1 = expert_1 == expert
        before = dot32(earlier, ones_where(named_0 | named_1))
        hit = before == (lane_id % cap).astype(jnp.float32)
        quarter = (lane_id // cap) % quarters
        block = source[slot].reshape(span, lanes)
        for q in range(quarters):
            here = hit & (quarter == q)
            picker = jnp.concatenate(
                [ones_where(named_0 & here), ones_where(named_1 & here)], axis=0
            )
            picked = dot32(picker, block)
            total[:, q * lanes : (q + 1) * lanes] += (
                picked[:rows] * weight_0 + picked[rows:] * weight_1
            )

    combine(0, yr, own)
    arrival = [2 * int(step[1]) + h for step in agenda if step[0] == "k" for h in range(2)]
    for slot in arrival:
        if slot == own:
            continue
        wait_bytes(xr.at[slot], xr_sem.at[slot], f"xr_{slot}")
        combine(offset(slot), xr, slot)
    expert_out[...] = total[...].astype(jnp.bfloat16)

    halo.wait_send()
    wait_bytes(xs.at[pl.ds(0, n_tp - 1)], xs_sem)
    wait_bytes(yd.at[:, pl.ds(0, n_ep - 1)], yf_sem)
    wait_bytes(ys.at[:, pl.ds(0, n_ep - 1)], ys_sem)
    wait_bytes(yr.at[pl.ds(0, n_tp - 1)], xb_sem)
    for step in range(1, half + 1):
        ring(step, 1).wait_send()
        if step < half:
            ring(step, -1).wait_send()


def held(array):
    return pltpu.with_memory_space_constraint(array, pltpu.HBM)


def on_device(
    pool_input,
    pool_map,
    pool_scale,
    out_weight,
    expert_input,
    norm_gain,
    routes,
    route_weight,
    gate_weight,
    up_weight,
    down_weight,
):
    n_ep, n_tp = lax.axis_size("ep"), lax.axis_size("tp")
    rows, width = expert_input.shape
    positions, channels = pool_input.shape
    hidden = gate_weight.shape[2]
    features = out_weight.shape[1]
    cap = 2 * rows * routes.shape[1] // (n_ep * n_tp)
    quarters = block_rows // cap
    lanes = width // quarters
    span = n_ep * block_rows
    half = n_tp // 2
    vmem = pl.BlockSpec(memory_space=pltpu.VMEM)
    far = pl.BlockSpec(memory_space=pl.ANY)
    bf16, f32 = jnp.bfloat16, jnp.float32
    exchange = pltpu.VMEM((n_tp, n_ep, block_rows, lanes), bf16)
    dma = pltpu.SemaphoreType.DMA
    return pl.pallas_call(
        functools.partial(kernel, n_ep, n_tp, cap),
        out_shape=(
            jax.ShapeDtypeStruct((positions, features), bf16),
            jax.ShapeDtypeStruct((rows, width), bf16),
        ),
        in_specs=[far] * 11,
        out_specs=(vmem, vmem),
        scratch_shapes=[
            pltpu.VMEM((1, width), f32),
            pltpu.VMEM(routes.T.shape, jnp.int32),
            pltpu.VMEM(routes.T.shape, f32),
            pltpu.VMEM((1, channels), f32),
            pltpu.VMEM((rows, width), bf16),
            pltpu.VMEM((width, hidden), bf16),
            pltpu.VMEM((width, hidden), bf16),
            pltpu.VMEM((hidden, width), bf16),
            pltpu.VMEM((positions, channels), bf16),
            pltpu.VMEM((channels, channels), bf16),
            pltpu.VMEM(out_weight.shape, bf16),
            pltpu.VMEM((halo_depth, channels), bf16),
            pltpu.VMEM((quarters * rows, lanes), bf16),
            exchange,
            exchange,
            exchange,
            exchange,
            exchange,
            exchange,
            pltpu.VMEM((2 * n_ep * cap, width), bf16),
            pltpu.VMEM((span, span), bf16),
            pltpu.VMEM((span, span), bf16),
            pltpu.VMEM((rows, width), f32),
            pltpu.VMEM((positions + halo_depth, channels), f32),
            pltpu.VMEM((3, positions + halo_depth, channels), f32),
            pltpu.VMEM((n_tp, positions, channels), bf16),
            dma((11,)),
            dma((2,)),
            dma,
            dma((n_tp,)),
            dma,
            dma((half,)),
            dma,
            dma((n_tp,)),
            dma,
            dma((n_tp,)),
            dma((2, half)),
            dma((2, half)),
        ],
        compiler_params=pltpu.CompilerParams(
            collective_id=0, has_side_effects=True, vmem_limit_bytes=50 * 1024 * 1024
        ),
    )(
        *map(
            held,
            (
                expert_input,
                norm_gain.reshape(1, width),
                routes.T,
                route_weight.T,
                gate_weight,
                up_weight,
                down_weight,
                pool_input,
                pool_map,
                pool_scale.reshape(n_tp, 1, channels),
                out_weight,
            ),
        )
    )


def solution(mesh):
    return jax.shard_map(
        on_device,
        mesh=mesh,
        in_specs=(
            P(("grp", "ep"), "tp"),
            P(),
            P(),
            P(None, "tp"),
            P(("grp", "ep", "tp"), None),
            P(),
            P(("grp", "ep", "tp"), None),
            P(("grp", "ep", "tp"), None),
            P(("ep", "tp"), None, None),
            P(("ep", "tp"), None, None),
            P(("ep", "tp"), None, None),
        ),
        out_specs=(P(("grp", "ep"), "tp"), P(("grp", "ep", "tp"), None)),
        check_vma=False,
    )
```

```python
import functools

import jax
import jax.numpy as jnp
from jax import lax
from jax.experimental import pallas as pl
from jax.experimental.pallas import tpu as pltpu
from jax.sharding import PartitionSpec as P

MESH = pl.DeviceIdType.MESH
epsilon = 1e-06
halo_depth = 16
block_rows = 16
pairs = ((2, 6), (1, 7), (3, 5), (4, 0))
agenda = ("r0", "r1", "e0", "s1", "r2", "w1", "s2", "k0", "r3", "e2", "w2", "s3", "e3", "k2", "w3", "s4", "e1", "k3", "k1")


def dot32(a, b):
    return jnp.dot(a, b, preferred_element_type=jnp.float32)


def iota(shape, dim):
    return lax.broadcasted_iota(jnp.int32, shape, dim)


def ones_where(mask):
    return jnp.where(mask, 1.0, 0.0).astype(jnp.bfloat16)


def kernel(
    n_ep,
    n_tp,
    cap,
    x_hbm,
    gain_hbm,
    routes_hbm,
    weight_hbm,
    gate_hbm,
    up_hbm,
    down_hbm,
    pool_hbm,
    map_hbm,
    scale_hbm,
    proj_hbm,
    pool_out,
    expert_out,
    gain_ref,
    routes_ref,
    weight_ref,
    scale_ref,
    x_v,
    gate_v,
    up_v,
    down_v,
    pool_v,
    map_v,
    proj_v,
    halo_v,
    stacked,
    xs,
    xd,
    yd,
    ys,
    yr,
    xr,
    rows_v,
    perm,
    perm_t,
    total,
    ext,
    sums,
    gathered,
    local_sem,
    halo_sem,
    xs_sem,
    xd_sem,
    yf_sem,
    yd_sem,
    ys_sem,
    yr_sem,
    xb_sem,
    xr_sem,
    ring_send,
    ring_recv,
):
    ep = lax.axis_index("ep")
    tp = lax.axis_index("tp")
    half = n_tp // 2
    rows, width = x_v.shape
    quarters = block_rows // cap
    lanes = width // quarters
    span = n_ep * block_rows
    part = n_ep * cap

    own = [off for pair in pairs for off in pair].index(0)

    def offset(slot):
        return pairs[slot // 2][slot % 2]

    def twin(slot):
        return slot if slot // 2 == own // 2 else slot ^ 1

    barrier = pltpu.get_barrier_semaphore()
    for r in range(1, n_tp):
        pl.semaphore_signal(
            barrier, inc=1, device_id={"tp": lax.rem(tp + r, n_tp)}, device_id_type=MESH
        )

    def greet(r, carry):
        pl.semaphore_signal(
            barrier, inc=1, device_id={"ep": lax.rem(ep + r, n_ep)}, device_id_type=MESH
        )
        return carry

    lax.fori_loop(1, n_ep, greet, 0)

    moves = [
        (x_hbm, x_v),
        (gain_hbm, gain_ref),
        (routes_hbm, routes_ref),
        (pool_hbm, pool_v),
        (map_hbm.at[tp], map_v),
        (scale_hbm.at[tp], scale_ref),
        (gate_hbm.at[0], gate_v),
        (up_hbm.at[0], up_v),
        (down_hbm.at[0], down_v),
        (proj_hbm, proj_v),
        (weight_hbm, weight_ref),
    ]
    loads = [
        pltpu.make_async_copy(source, target, local_sem.at[n])
        for n, (source, target) in enumerate(moves)
    ]
    for load in loads:
        load.start()

    later = ones_where(iota((rows, rows), 0) < iota((rows, rows), 1))
    earlier = ones_where(iota((rows, rows), 0) > iota((rows, rows), 1))
    row_id, col_id = iota((span, span), 0), iota((span, span), 1)

    def home(v):
        return ((v // cap) % n_ep) * block_rows + (v // part) * cap + v % cap

    perm[...] = ones_where(home(row_id) == col_id)
    perm_t[...] = ones_where(row_id == home(col_id))

    for load in loads[:3]:
        load.wait()
    widened = x_v[...].astype(jnp.float32)
    normed = (
        widened
        * lax.rsqrt(jnp.mean(widened * widened, axis=1, keepdims=True) + epsilon)
        * gain_ref[...]
    ).astype(jnp.bfloat16)
    for q in range(quarters):
        stacked[q * rows : (q + 1) * rows, :] = normed[:, q * lanes : (q + 1) * lanes]

    slot_row = iota((span, rows), 0)

    def build(slot, off):
        expert = (slot_row // block_rows) * n_tp + lax.rem(tp + off, n_tp)
        named = (routes_ref[0:1, :] == expert) | (routes_ref[1:2, :] == expert)
        before = dot32(ones_where(named), later)
        chosen = named & (before == (slot_row % cap).astype(jnp.float32))
        quarter = (slot_row // cap) % quarters
        selector = jnp.concatenate(
            [ones_where(chosen & (quarter == q)) for q in range(quarters)], axis=1
        )
        block = dot32(selector, stacked[...]).astype(jnp.bfloat16)
        xs[slot] = block.reshape(n_ep, block_rows, lanes)

    def send_x(slot):
        pltpu.make_async_remote_copy(
            src_ref=xs.at[slot],
            dst_ref=xd.at[twin(slot)],
            send_sem=xs_sem,
            recv_sem=xd_sem.at[twin(slot)],
            device_id={"tp": lax.rem(tp + offset(slot), n_tp)},
            device_id_type=MESH,
        ).start()

    def forward_y(slot, source):
        def one(r, carry):
            peer = lax.rem(ep + r, n_ep)
            pltpu.make_async_remote_copy(
                src_ref=source.at[slot, peer],
                dst_ref=yd.at[slot, ep],
                send_sem=yf_sem,
                recv_sem=yd_sem.at[slot // 2],
                device_id={"ep": peer},
                device_id_type=MESH,
            ).start()
            return carry

        lax.fori_loop(1, n_ep, one, 0)
        yd[slot, ep] = source[slot, ep]

    def wait_bytes(ref, sem, name="drain"):
        with jax.named_scope(name):
            pltpu.make_async_copy(ref, ref, sem).wait()

    order = [slot for slot in range(n_tp) if slot != own]
    build(order[0], offset(order[0]))
    with jax.named_scope("barrier"):
        pl.semaphore_wait(barrier, n_tp - 1 + n_ep - 1)
    halo = pltpu.make_async_remote_copy(
        src_ref=pool_v.at[pool_v.shape[0] - halo_depth :],
        dst_ref=halo_v,
        send_sem=halo_sem.at[0],
        recv_sem=halo_sem.at[1],
        device_id={"ep": lax.rem(ep + 1, n_ep)},
        device_id_type=MESH,
    )
    build(order[1], offset(order[1]))
    send_x(order[0])
    build(own, 0)
    send_x(order[1])
    loads[3].wait()
    halo.start()
    build(order[2], offset(order[2]))
    forward_y(own, xs)
    for n in range(3, len(order)):
        build(order[n], offset(order[n]))
        send_x(order[n - 1])
    send_x(order[-1])

    for load in loads[4:6]:
        load.wait()
    positions, channels = pool_v.shape
    ext[halo_depth:, :] = pool_v[...].astype(jnp.float32)
    with jax.named_scope("halo"):
        halo.wait_recv()
    halo_rows = halo_v[...].astype(jnp.float32)
    ext[0:halo_depth, :] = jnp.where(ep == 0, jnp.zeros_like(halo_rows), halo_rows)
    level = lax.rem(tp, 4)
    summed = ext[halo_depth:, :] + ext[halo_depth - 1 : -1, :]
    sums[0, halo_depth:, :] = summed
    sums[0, 1:halo_depth, :] = ext[1:halo_depth, :] + ext[0 : halo_depth - 1, :]
    reach = 2
    first = 1
    for n in range(3):
        first = first + reach
        wider = sums[n, first:, :] + sums[n, first - reach : -reach, :]
        if n < 2:
            sums[n + 1, first:, :] = wider
        summed = jnp.where(level > n, wider[halo_depth - first :], summed)
        reach = 2 * reach
    window = jnp.left_shift(2, level)
    position = ep * positions + iota((positions, channels), 0)
    counted = jnp.minimum(position + 1, window).astype(jnp.float32)
    pooled = (summed / counted - ext[halo_depth:, :]).astype(jnp.bfloat16)
    mapped = dot32(pooled, map_v[...]) * scale_ref[...]
    gathered[tp] = mapped.astype(jnp.bfloat16)

    def ring(step, way):
        block = lax.rem(tp + n_tp - way * (step - 1), n_tp)
        lane = (1 - way) // 2
        return pltpu.make_async_remote_copy(
            src_ref=gathered.at[block],
            dst_ref=gathered.at[block],
            send_sem=ring_send.at[lane, step - 1],
            recv_sem=ring_recv.at[lane, step - 1],
            device_id={"tp": lax.rem(tp + n_tp + way, n_tp)},
            device_id_type=MESH,
        )

    def relay(b):
        for slot in (2 * b, 2 * b + 1):
            if slot != own:
                wait_bytes(xd.at[slot], xd_sem.at[slot], f"xd_{slot}")
                forward_y(slot, xd)

    def send_back(b):
        for slot in (2 * b, 2 * b + 1):
            wait_bytes(yr.at[slot, pl.ds(0, n_ep - 1)], yr_sem.at[slot], f"yr_{slot}")
            if slot != own:
                pltpu.make_async_remote_copy(
                    src_ref=yr.at[slot],
                    dst_ref=xr.at[twin(slot)],
                    send_sem=xb_sem,
                    recv_sem=xr_sem.at[twin(slot)],
                    device_id={"tp": lax.rem(tp + offset(slot), n_tp)},
                    device_id_type=MESH,
                ).start()

    def experts(b):
        wait_bytes(yd.at[pl.ds(2 * b, 2), pl.ds(0, n_ep - 1)], yd_sem.at[b], f"yd_{b}")
        for h in range(2):
            block = yd[2 * b + h].reshape(span, lanes)
            ordered = dot32(perm[...], block).astype(jnp.bfloat16)
            for q in range(quarters):
                rows_v[h * part : (h + 1) * part, q * lanes : (q + 1) * lanes] = ordered[
                    q * part : (q + 1) * part, :
                ]
        gate = dot32(rows_v[...], gate_v[...])
        up = dot32(rows_v[...], up_v[...])
        hidden = (gate / (1.0 + jnp.exp(-gate)) * up).astype(jnp.bfloat16)
        result = dot32(hidden, down_v[...]).astype(jnp.bfloat16)
        for h in range(2):
            tall = jnp.concatenate(
                [
                    result[h * part : (h + 1) * part, q * lanes : (q + 1) * lanes]
                    for q in range(quarters)
                ],
                axis=0,
            )
            block = dot32(perm_t[...], tall).astype(jnp.bfloat16)
            ys[2 * b + h] = block.reshape(n_ep, block_rows, lanes)
        for h in range(2):
            yr[2 * b + h, ep] = ys[2 * b + h, ep]

        def one(n, c):
            h = n // (n_ep - 1)
            peer = lax.rem(ep + 1 + n - h * (n_ep - 1), n_ep)
            pltpu.make_async_remote_copy(
                src_ref=ys.at[2 * b + h, peer],
                dst_ref=yr.at[2 * b + h, ep],
                send_sem=ys_sem,
                recv_sem=yr_sem.at[2 * b + h],
                device_id={"ep": peer},
                device_id_type=MESH,
            ).start()
            return c

        lax.fori_loop(0, 2 * (n_ep - 1), one, 0)

    def ring_start(step):
        ring(step, 1).start()
        if step < half:
            ring(step, -1).start()

    def ring_wait(step):
        with jax.named_scope(f"ring_{step}"):
            ring(step, 1).wait_recv()
            if step < half:
                ring(step, -1).wait_recv()

    for load in loads[6:]:
        load.wait()
    calls = {
        "r": relay,
        "e": experts,
        "k": send_back,
        "s": ring_start,
        "w": ring_wait,
    }
    for step in agenda:
        calls[step[0]](int(step[1]))

    tile = positions // 4

    def project(n, carry):
        at = pl.ds(pl.multiple_of(n * tile, tile), tile)
        left = jnp.concatenate([gathered[j, at, :] for j in range(n_tp)], axis=1)
        pool_out[at, :] = dot32(left, proj_v[...]).astype(jnp.bfloat16)
        return carry


    total[...] = jnp.zeros_like(total)
    lane_id = iota((rows, span), 1)

    def upright(ref, k):
        return jnp.broadcast_to(ref[k : k + 1, :], (rows, rows)).T[:, 0:1]

    expert_0, expert_1 = upright(routes_ref, 0), upright(routes_ref, 1)
    weight_0, weight_1 = upright(weight_ref, 0), upright(weight_ref, 1)

    def combine(off, source, slot):
        expert = (lane_id // block_rows) * n_tp + lax.rem(tp + off, n_tp)
        named_0 = expert_0 == expert
        named_1 = expert_1 == expert
        before = dot32(earlier, ones_where(named_0 | named_1))
        hit = before == (lane_id % cap).astype(jnp.float32)
        quarter = (lane_id // cap) % quarters
        block = source[slot].reshape(span, lanes)
        for q in range(quarters):
            here = hit & (quarter == q)
            picker = jnp.concatenate(
                [ones_where(named_0 & here), ones_where(named_1 & here)], axis=0
            )
            picked = dot32(picker, block)
            total[:, q * lanes : (q + 1) * lanes] += (
                picked[:rows] * weight_0 + picked[rows:] * weight_1
            )

    combine(0, yr, own)
    arrival = [2 * int(step[1]) + h for step in agenda if step[0] == "k" for h in range(2)]
    for slot in arrival:
        if slot == own:
            continue
        if slot == arrival[-4]:
            ring_wait(half)
            lax.fori_loop(0, 4, project, 0)
        wait_bytes(xr.at[slot], xr_sem.at[slot], f"xr_{slot}")
        combine(offset(slot), xr, slot)
    expert_out[...] = total[...].astype(jnp.bfloat16)

    halo.wait_send()
    wait_bytes(xs.at[pl.ds(0, n_tp - 1)], xs_sem)
    wait_bytes(yd.at[:, pl.ds(0, n_ep - 1)], yf_sem)
    wait_bytes(ys.at[:, pl.ds(0, n_ep - 1)], ys_sem)
    wait_bytes(yr.at[pl.ds(0, n_tp - 1)], xb_sem)
    for step in range(1, half + 1):
        ring(step, 1).wait_send()
        if step < half:
            ring(step, -1).wait_send()


def held(array):
    return pltpu.with_memory_space_constraint(array, pltpu.HBM)


def on_device(
    pool_input,
    pool_map,
    pool_scale,
    out_weight,
    expert_input,
    norm_gain,
    routes,
    route_weight,
    gate_weight,
    up_weight,
    down_weight,
):
    n_ep, n_tp = lax.axis_size("ep"), lax.axis_size("tp")
    rows, width = expert_input.shape
    positions, channels = pool_input.shape
    hidden = gate_weight.shape[2]
    features = out_weight.shape[1]
    cap = 2 * rows * routes.shape[1] // (n_ep * n_tp)
    quarters = block_rows // cap
    lanes = width // quarters
    span = n_ep * block_rows
    half = n_tp // 2
    vmem = pl.BlockSpec(memory_space=pltpu.VMEM)
    far = pl.BlockSpec(memory_space=pl.ANY)
    bf16, f32 = jnp.bfloat16, jnp.float32
    exchange = pltpu.VMEM((n_tp, n_ep, block_rows, lanes), bf16)
    dma = pltpu.SemaphoreType.DMA
    return pl.pallas_call(
        functools.partial(kernel, n_ep, n_tp, cap),
        out_shape=(
            jax.ShapeDtypeStruct((positions, features), bf16),
            jax.ShapeDtypeStruct((rows, width), bf16),
        ),
        in_specs=[far] * 11,
        out_specs=(vmem, vmem),
        scratch_shapes=[
            pltpu.VMEM((1, width), f32),
            pltpu.VMEM(routes.T.shape, jnp.int32),
            pltpu.VMEM(routes.T.shape, f32),
            pltpu.VMEM((1, channels), f32),
            pltpu.VMEM((rows, width), bf16),
            pltpu.VMEM((width, hidden), bf16),
            pltpu.VMEM((width, hidden), bf16),
            pltpu.VMEM((hidden, width), bf16),
            pltpu.VMEM((positions, channels), bf16),
            pltpu.VMEM((channels, channels), bf16),
            pltpu.VMEM(out_weight.shape, bf16),
            pltpu.VMEM((halo_depth, channels), bf16),
            pltpu.VMEM((quarters * rows, lanes), bf16),
            exchange,
            exchange,
            exchange,
            exchange,
            exchange,
            exchange,
            pltpu.VMEM((2 * n_ep * cap, width), bf16),
            pltpu.VMEM((span, span), bf16),
            pltpu.VMEM((span, span), bf16),
            pltpu.VMEM((rows, width), f32),
            pltpu.VMEM((positions + halo_depth, channels), f32),
            pltpu.VMEM((3, positions + halo_depth, channels), f32),
            pltpu.VMEM((n_tp, positions, channels), bf16),
            dma((11,)),
            dma((2,)),
            dma,
            dma((n_tp,)),
            dma,
            dma((half,)),
            dma,
            dma((n_tp,)),
            dma,
            dma((n_tp,)),
            dma((2, half)),
            dma((2, half)),
        ],
        compiler_params=pltpu.CompilerParams(
            collective_id=0, has_side_effects=True, vmem_limit_bytes=50 * 1024 * 1024
        ),
    )(
        *map(
            held,
            (
                expert_input,
                norm_gain.reshape(1, width),
                routes.T,
                route_weight.T,
                gate_weight,
                up_weight,
                down_weight,
                pool_input,
                pool_map,
                pool_scale.reshape(n_tp, 1, channels),
                out_weight,
            ),
        )
    )


def solution(mesh):
    return jax.shard_map(
        on_device,
        mesh=mesh,
        in_specs=(
            P(("grp", "ep"), "tp"),
            P(),
            P(),
            P(None, "tp"),
            P(("grp", "ep", "tp"), None),
            P(),
            P(("grp", "ep", "tp"), None),
            P(("grp", "ep", "tp"), None),
            P(("ep", "tp"), None, None),
            P(("ep", "tp"), None, None),
            P(("ep", "tp"), None, None),
        ),
        out_specs=(P(("grp", "ep"), "tp"), P(("grp", "ep", "tp"), None)),
        check_vma=False,
    )
```
